128 devices in a mesh: sp: 16 (over z, x), tp: 8 (over y, core).
Axes of the slice: x: 4, y: 4, z: 4, core: 2. Of those that a mesh axis runs over, the one named last changes fastest.
Arguments:
- latent: bfloat16 [8192, 4096], P('sp'), may hold values from -64 to 64
- context: bfloat16 [1024, 4096], P('sp'), may hold values from -6 to 6
- condition: bfloat16 [4096], P('sp'), may hold values from -6 to 6
- context_condition: bfloat16 [4096], P('sp'), may hold values from -6 to 6
- shift_weight: bfloat16 [4096, 4096], P('sp', 'tp'), may hold values from -0.125 to 0.125
- scale_weight: bfloat16 [4096, 4096], P('sp', 'tp'), may hold values from -0.125 to 0.125
- gate_weight: bfloat16 [4096, 4096], P('sp', 'tp'), may hold values from -0.25 to 0.25
- norm_gain: float32 [4096], replicated, may hold values from 0.1 to 1.9
- query_weight: bfloat16 [4096, 2048], P(None, 'tp'), may hold values from -0.09375 to 0.09375
- key_weight: bfloat16 [4096, 2048], P(None, 'tp'), may hold values from -0.09375 to 0.09375
- value_weight: bfloat16 [4096, 2048], P(None, 'tp'), may hold values from -0.09375 to 0.09375
- write_weight: bfloat16 [4096, 2, 16], replicated, may hold values from -0.09375 to 0.09375
- decay_weight: bfloat16 [4096, 2, 16], replicated, may hold values from -0.09375 to 0.09375
- write_bias: float32 [2, 16], replicated, may hold values from -12 to 1
- decay_bias: float32 [2, 16], replicated, may hold values from -16 to -4
- log_rate: float32 [2, 16], replicated, may hold values from 0 to 1.4
- head_gain: float32 [128], replicated, may hold values from 0.1 to 1.9
- out_weight: bfloat16 [2048, 4096], P(None, 'tp'), may hold values from -0.125 to 0.125
Outputs:
- updated: bfloat16 [8192, 4096], P('sp', 'tp')
The draws below stay inside these ranges and needn't reach their ends.
All inputs are finite; a program needn't handle non-finite values.
Results may differ from the reference program's by a relative error of at most 0.013.
Values may be sent and summed in bfloat16 or wider, within the bound.
No kernel may reach another device: no remote copies, remote signals or barrier semaphores. Data moves between devices by JAX's collectives and lax.ppermute only.
A program may use at most 128 MiB of HBM per device.

```python
import math
import jax
import jax.numpy as jnp
from jax import lax

D = 4096
HEADS = 16
HEAD_DIM = 128
BLOCK = 64
TOKENS = 8192
CTX = 1024


def draw_latent(key, part):
    segment_count = (TOKENS + 127) // 128
    offsets = jnp.clip(jax.random.normal(jax.random.fold_in(key, 22), (segment_count, D), jnp.float32), -3.0, 3.0)
    segment_index = jnp.arange(TOKENS) // 128
    noise = jnp.clip(jax.random.normal(jax.random.fold_in(key, 21), (TOKENS, D), jnp.float32), -6.0, 6.0)
    return (noise + offsets[segment_index]).astype(jnp.bfloat16)


def head_speeds(key):
    chooser = jax.random.uniform(jax.random.fold_in(key, 31), (2, HEADS), jnp.float32)
    return chooser < 0.7


def draw_decay_bias(key, part):
    keeping = head_speeds(key)
    spread = jax.random.uniform(jax.random.fold_in(key, 32), (2, HEADS), jnp.float32, -0.5, 0.5)
    slow_value = math.log(0.05 / (TOKENS + CTX)) + spread
    fast_value = -5.0 + spread
    return jnp.where(keeping, slow_value, fast_value).astype(jnp.float32)


def draw_write_bias(key, part):
    keeping = head_speeds(key)
    spread = jax.random.uniform(jax.random.fold_in(key, 33), (2, HEADS), jnp.float32, -0.5, 0.5)
    slow_value = math.log(HEAD_DIM / (TOKENS + CTX)) - 1.5 + spread
    fast_value = spread
    return jnp.where(keeping, slow_value, fast_value).astype(jnp.float32)


def block_levels(rng, shape, cuts, least, high):
    level = 1.0
    for position, blocks in cuts:
        draws = jax.random.uniform(jax.random.fold_in(jax.random.fold_in(rng, 6), position), (blocks,), jnp.float32, least / len(cuts), high / len(cuts))
        level = level * jnp.repeat(jnp.exp(draws), shape[position] // blocks).reshape((-1,) + (1,) * (len(shape) - 1 - position))
    return level


def gaussian(key, extent, scale, most, split=(), held_as=jnp.bfloat16):
    drawn = jax.random.normal(key, extent, jnp.float32) * scale
    if len(split) > 0:
        drawn = block_levels(key, extent, split, -0.22, 0.18) * drawn
    return jnp.clip(drawn, min=-most, max=most).astype(held_as)


def setup_inputs(seed: int = 0) -> dict:
    keys = jax.random.split(jax.random.key(seed), 19)
    return {
        "latent": draw_latent(jax.random.fold_in(keys[18], 71), 0),
        "context": gaussian(keys[1], (CTX, D), 1.0, 6.0, ((0, 16),)),
        "condition": gaussian(keys[2], (D,), 1.0, 6.0, ((0, 16),)),
        "context_condition": gaussian(keys[3], (D,), 1.0, 6.0, ((0, 16),)),
        "shift_weight": gaussian(keys[4], (D, D), (D // 2) ** -0.5, 0.125, ((0, 16), (1, 8))),
        "scale_weight": gaussian(keys[5], (D, D), (D // 2) ** -0.5, 0.125, ((0, 16), (1, 8))),
        "gate_weight": gaussian(keys[6], (D, D), (D // 8) ** -0.5, 0.25, ((0, 16), (1, 8))),
        "norm_gain": jnp.clip(1.0 + 0.18 * jax.random.normal(keys[7], (D,), jnp.float32), 0.1, 1.9),
        "query_weight": gaussian(keys[8], (D, HEADS * HEAD_DIM), D ** -0.5, 0.09375, ((1, 8),)),
        "key_weight": gaussian(keys[9], (D, HEADS * HEAD_DIM), D ** -0.5, 0.09375, ((1, 8),)),
        "value_weight": gaussian(keys[10], (D, HEADS * HEAD_DIM), D ** -0.5, 0.09375, ((1, 8),)),
        "write_weight": gaussian(keys[11], (D, 2, HEADS), D ** -0.5, 0.09375),
        "decay_weight": gaussian(keys[12], (D, 2, HEADS), D ** -0.5, 0.09375),
        "write_bias": draw_write_bias(jax.random.fold_in(keys[18], 71), 0),
        "decay_bias": draw_decay_bias(jax.random.fold_in(keys[18], 71), 0),
        "log_rate": jnp.clip(jax.random.uniform(keys[15], (2, HEADS), jnp.float32, 0.0, 1.4), 0.0, 1.4),
        "head_gain": jnp.clip(1.0 + 0.18 * jax.random.normal(keys[16], (HEAD_DIM,), jnp.float32), 0.1, 1.9),
        "out_weight": gaussian(keys[17], (HEADS * HEAD_DIM, D), (HEADS * HEAD_DIM) ** -0.5, 0.125, ((1, 8),)),
    }


epsilon = 0.0001
highest = lax.Precision.HIGHEST

def rms_rows(row_data, row_gain):
    values = row_data.astype(jnp.float32)
    scaled = values * lax.rsqrt(lax.optimization_barrier(jnp.mean(values * values, axis=-1, keepdims=True)) + epsilon)
    return scaled * row_gain.astype(jnp.float32)

def unit_heads(matrix, head_count):
    split_heads = matrix.astype(jnp.float32).reshape(matrix.shape[0], head_count, -1)
    return split_heads * lax.rsqrt(lax.optimization_barrier(jnp.sum(split_heads * split_heads, axis=-1, keepdims=True)) + epsilon)

def head_gates(write_pre, decay_pre, write_bias, decay_bias, log_rate):
    write_rate = jax.nn.sigmoid(write_pre.astype(jnp.float32) + write_bias)
    log_decay = -jnp.exp(log_rate) * jax.nn.softplus(decay_pre.astype(jnp.float32) + decay_bias)
    return (write_rate, log_decay)

def project(matrix, weight):
    return jnp.dot(matrix.astype(jnp.float32), weight.astype(jnp.float32), preferred_element_type=jnp.float32).astype(jnp.bfloat16)

def to_blocks(source):
    heads_first = jnp.moveaxis(source, 1, 0)
    block_count = heads_first.shape[1] // BLOCK
    return heads_first.reshape((heads_first.shape[0], block_count, BLOCK) + heads_first.shape[2:])

def prepare_keys(key_vecs, value_vecs, log_decay, write_rate):
    block_keys = to_blocks(key_vecs)
    block_values = to_blocks(value_vecs)
    running = jnp.cumsum(to_blocks(log_decay), axis=-1)
    block_rates = to_blocks(write_rate)
    offsets = jnp.arange(BLOCK)
    lower_mask = offsets[:, None] >= offsets[None, :]
    strict_mask = offsets[:, None] > offsets[None, :]
    spread = running[..., :, None] - running[..., None, :]
    decay_mat = jnp.where(lower_mask, jnp.exp(jnp.where(lower_mask, spread, 0.0)), 0.0)
    scaled = block_keys * block_rates[..., None]
    system = jnp.einsum('hnid,hnjd->hnij', scaled, block_keys, precision=highest) * decay_mat
    system = jnp.where(strict_mask, system, 0.0) + jnp.eye(BLOCK, dtype=system.dtype)
    fresh_values = jax.scipy.linalg.solve_triangular(system, block_values * block_rates[..., None], lower=True, unit_diagonal=True)
    key_weights = jax.scipy.linalg.solve_triangular(system, scaled * jnp.exp(running)[..., None], lower=True, unit_diagonal=True)
    last_gate = running[..., -1]
    late_keys = block_keys * jnp.exp(last_gate[..., None] - running)[..., None]
    return (block_keys, running, decay_mat, fresh_values, key_weights, last_gate, late_keys)

def prepare_queries(query_vecs, prepared):
    block_queries = to_blocks(query_vecs)
    query_keys = jnp.einsum('hnid,hnjd->hnij', block_queries, prepared[0], precision=highest) * prepared[2]
    early_queries = block_queries * jnp.exp(prepared[1])[..., None]
    return (query_keys, early_queries)

def run_blocks(prepared, queried, start):
    inputs = tuple((jnp.moveaxis(item, 1, 0) for item in (prepared[3], prepared[4], queried[0], queried[1], prepared[6], prepared[5])))

    def advance(carried, pieces):
        new_in, key_in, score_in, query_in, late_in, gate_in = pieces
        corrected = new_in - jnp.einsum('hcd,hde->hce', key_in, carried, precision=highest)
        output = jnp.einsum('hcd,hde->hce', query_in, carried, precision=highest)
        output = output + jnp.einsum('hij,hje->hie', score_in, corrected, precision=highest)
        carried = carried * jnp.exp(gate_in)[:, None, None] + jnp.einsum('hcd,hce->hde', late_in, corrected, precision=highest)
        return (carried, output)
    closing, outputs = lax.scan(advance, start, inputs)
    merged = jnp.transpose(outputs, (0, 2, 1, 3))
    return merged.reshape(-1, merged.shape[2], merged.shape[3])

def final_state(prepared, start):
    inputs = tuple((jnp.moveaxis(item, 1, 0) for item in (prepared[3], prepared[4], prepared[6], prepared[5])))

    def advance(carried, pieces):
        new_in, key_in, late_in, gate_in = pieces
        corrected = new_in - jnp.einsum('hcd,hde->hce', key_in, carried, precision=highest)
        carried = carried * jnp.exp(gate_in)[:, None, None] + jnp.einsum('hcd,hce->hde', late_in, corrected, precision=highest)
        return (carried, None)
    closing, unused = lax.scan(advance, start, inputs)
    return closing

def reference(latent, context, condition, context_condition, shift_weight, scale_weight, gate_weight, norm_gain, query_weight, key_weight, value_weight, write_weight, decay_weight, write_bias, decay_bias, log_rate, head_gain, out_weight):
    head_count = write_bias.shape[1]
    width = write_weight.shape[0]
    stacked = jnp.stack([condition, context_condition]).astype(jnp.float32)
    silu_rows = jax.nn.silu(stacked).astype(jnp.bfloat16)
    shift_rows = jnp.dot(silu_rows.astype(jnp.float32), shift_weight.astype(jnp.float32), preferred_element_type=jnp.float32)
    scale_rows = jnp.dot(silu_rows.astype(jnp.float32), scale_weight.astype(jnp.float32), preferred_element_type=jnp.float32)
    gate_row = jnp.dot(silu_rows[0].astype(jnp.float32), gate_weight.astype(jnp.float32), preferred_element_type=jnp.float32)
    modulated = (rms_rows(latent, norm_gain) * (1.0 + scale_rows[0]) + shift_rows[0]).astype(jnp.bfloat16)
    ctx_modulated = (rms_rows(context, norm_gain) * (1.0 + scale_rows[1]) + shift_rows[1]).astype(jnp.bfloat16)
    write_flat = write_weight.reshape(width, -1)
    decay_flat = decay_weight.reshape(width, -1)
    ctx_keys = unit_heads(project(ctx_modulated, key_weight), head_count)
    ctx_values = project(ctx_modulated, value_weight).astype(jnp.float32).reshape(-1, head_count, HEAD_DIM)
    ctx_rate, ctx_log = head_gates(project(ctx_modulated, write_flat).reshape(-1, 2, head_count), project(ctx_modulated, decay_flat).reshape(-1, 2, head_count), write_bias, decay_bias, log_rate)
    start_zero = jnp.zeros((head_count, HEAD_DIM, HEAD_DIM), jnp.float32)
    ctx_forward = final_state(prepare_keys(ctx_keys, ctx_values, ctx_log[:, 0], ctx_rate[:, 0]), start_zero)
    ctx_backward = final_state(prepare_keys(jnp.flip(ctx_keys, 0), jnp.flip(ctx_values, 0), jnp.flip(ctx_log[:, 1], 0), jnp.flip(ctx_rate[:, 1], 0)), start_zero)
    queries = unit_heads(project(modulated, query_weight), head_count) * HEAD_DIM ** (-0.5)
    key_vecs = unit_heads(project(modulated, key_weight), head_count)
    value_vecs = project(modulated, value_weight).astype(jnp.float32).reshape(-1, head_count, HEAD_DIM)
    write_rate, log_decay = head_gates(project(modulated, write_flat).reshape(-1, 2, head_count), project(modulated, decay_flat).reshape(-1, 2, head_count), write_bias, decay_bias, log_rate)
    forward_prep = prepare_keys(key_vecs, value_vecs, log_decay[:, 0], write_rate[:, 0])
    forward_out = run_blocks(forward_prep, prepare_queries(queries, forward_prep), ctx_forward)
    backward_prep = prepare_keys(jnp.flip(key_vecs, 0), jnp.flip(value_vecs, 0), jnp.flip(log_decay[:, 1], 0), jnp.flip(write_rate[:, 1], 0))
    backward_out = jnp.flip(run_blocks(backward_prep, prepare_queries(jnp.flip(queries, 0), backward_prep), ctx_backward), 0)
    combined = forward_out + backward_out
    head_out = combined * lax.rsqrt(lax.optimization_barrier(jnp.mean(combined * combined, axis=-1, keepdims=True)) + epsilon) * head_gain.astype(jnp.float32)
    head_out = head_out.astype(jnp.bfloat16).reshape(combined.shape[0], -1)
    branch = jnp.dot(head_out.astype(jnp.float32), out_weight.astype(jnp.float32), preferred_element_type=jnp.float32)
    return (latent.astype(jnp.float32) + gate_row * branch).astype(jnp.bfloat16)
```

```python
import functools

import jax
import jax.numpy as jnp
from jax import lax
from jax.experimental import pallas as pl
from jax.experimental.pallas import tpu as pltpu
from jax.sharding import Mesh
from jax.sharding import PartitionSpec as P

HEAD_DIM = 128
BLOCK = 128
SP = ("z", "x")
TP = ("y", "c")
ALL = ("z", "x", "y", "c")
SLICE = 32
EPS = 0.0001
F32 = jnp.float32
BF16 = jnp.bfloat16


def dot(a, b):
    return jnp.dot(a, b, preferred_element_type=F32)


def dot_t(a, b):
    return lax.dot_general(a, b, (((1,), (1,)), ((), ())), preferred_element_type=F32)


def t_dot(a, b):
    return lax.dot_general(a, b, (((0,), (0,)), ((), ())), preferred_element_type=F32)


def exact_dot(a, b):
    return jnp.dot(a, b, preferred_element_type=F32, precision=lax.Precision.HIGHEST)


def iotas(n):
    shape = (n, n)
    return lax.broadcasted_iota(jnp.int32, shape, 0), lax.broadcasted_iota(jnp.int32, shape, 1)


def unit(x):
    x = x.astype(F32)
    return x * lax.rsqrt(jnp.sum(x * x, axis=-1, keepdims=True) + EPS)


def log1p_small(e):
    series = e * (1.0 - e * (0.5 - e * (1.0 / 3.0 - 0.25 * e)))
    return jnp.where(e < 0.01, series, jnp.log(1.0 + e))


def softplus(x):
    return jnp.maximum(x, 0.0) + log1p_small(jnp.exp(-jnp.abs(x)))


def row_scale_kernel(lat_ref, ctx_ref, lat_out, ctx_out):
    def scale(ref):
        x = ref[...].astype(F32)
        s = lax.rsqrt(jnp.mean(x * x, axis=-1, keepdims=True) + EPS)
        return jnp.broadcast_to(s, (x.shape[0], 128))

    lat_out[...] = scale(lat_ref)

    @pl.when(pl.program_id(0) == 0)
    def _():
        ctx_out[...] = scale(ctx_ref)


def row_scales(latent, context):
    rows, width = latent.shape
    crows = context.shape[0]
    step = 128
    return pl.pallas_call(
        row_scale_kernel,
        grid=(rows // step,),
        in_specs=[
            pl.BlockSpec((step, width), lambda i: (i, 0)),
            pl.BlockSpec((crows, width), lambda i: (0, 0)),
        ],
        out_specs=[
            pl.BlockSpec((step, 128), lambda i: (i, 0)),
            pl.BlockSpec((crows, 128), lambda i: (0, 0)),
        ],
        out_shape=[
            jax.ShapeDtypeStruct((rows, 128), F32),
            jax.ShapeDtypeStruct((crows, 128), F32),
        ],
        name="row_scales",
    )(latent, context)


def project_kernel(
    recv_ref, gain_ref, lat_ref, ctx_ref, ls_ref, cs_ref, wq, wk, wv, wg, q_out, k_out, v_out, g_out, acc
):
    step = pl.program_id(0)
    rows = lat_ref.shape[0]
    sums = jnp.sum(recv_ref[...].astype(F32), axis=0)[0]
    gain = gain_ref[...]
    width = lat_ref.shape[1]

    def modulate(ref, scale_ref, r):
        x = ref[...].astype(F32)
        s = jnp.concatenate([scale_ref[...]] * (width // 128), axis=1)
        normed = x * s * gain
        return (normed * (1.0 + sums[2 + r : 3 + r]) + sums[r : r + 1]).astype(BF16)

    m = jnp.concatenate([modulate(lat_ref, ls_ref, 0), modulate(ctx_ref, cs_ref, 1)], axis=0)

    at = 0
    for w in (wq, wk, wv, wg):
        n = w.shape[1]
        part = dot(m, w[...])

        @pl.when(step == 0)
        def _():
            acc[:, at : at + n] = part

        @pl.when(step > 0)
        def _():
            acc[:, at : at + n] += part

        at += n

    @pl.when(step == pl.num_programs(0) - 1)
    def _():
        at = 0
        for o in (q_out, k_out, v_out, g_out):
            n = o.shape[1]
            o[...] = acc[: o.shape[0], at : at + n].astype(BF16)
            at += n


def projections(recv, gain, latent, context, ls, cs, wq, wk, wv, wg):
    rows, width = latent.shape
    crows = context.shape[0]
    every = rows + crows
    peers, parts, five, step = recv.shape
    ncol = wq.shape[1]
    gcol = wg.shape[1]
    col = lambda i: (0, i)
    row = lambda i: (i, 0)
    one = lambda i: (0, 0)
    return pl.pallas_call(
        project_kernel,
        grid=(parts,),
        in_specs=[
            pl.BlockSpec((peers, 1, five, step), lambda i: (0, i, 0, 0)),
            pl.BlockSpec((1, step), col),
            pl.BlockSpec((rows, step), col),
            pl.BlockSpec((crows, step), col),
            pl.BlockSpec((rows, 128), one),
            pl.BlockSpec((crows, 128), one),
            pl.BlockSpec((step, ncol), row),
            pl.BlockSpec((step, ncol), row),
            pl.BlockSpec((step, ncol), row),
            pl.BlockSpec((step, gcol), row),
        ],
        out_specs=[
            pl.BlockSpec((rows, ncol), one),
            pl.BlockSpec((every, ncol), one),
            pl.BlockSpec((every, ncol), one),
            pl.BlockSpec((every, gcol), one),
        ],
        out_shape=[
            jax.ShapeDtypeStruct((rows, ncol), BF16),
            jax.ShapeDtypeStruct((every, ncol), BF16),
            jax.ShapeDtypeStruct((every, ncol), BF16),
            jax.ShapeDtypeStruct((every, gcol), BF16),
        ],
        scratch_shapes=[pltpu.VMEM((every, 3 * ncol + gcol), F32)],
        name="projections",
    )(recv, gain, latent, context, ls, cs, wq, wk, wv, wg)


def maps_kernel(
    k_ref, v_ref, g_ref, bias_ref, log_rate_ref, send_ref, sv_ref, gates_ref, low, inv, uw
):
    nblk = (k_ref.shape[0] - 64) // BLOCK
    lats = nblk * BLOCK
    ri, ci = iotas(BLOCK)
    apart = ri ^ ci
    eye = (ri == ci).astype(F32)
    pre = g_ref[...].astype(F32) + bias_ref[...]
    rates = jax.nn.sigmoid(pre)
    logs = -jnp.exp(log_rate_ref[...]) * softplus(pre)
    lower = (ri >= ci).astype(F32)
    upper = (ri <= ci).astype(F32)
    strict = (ri > ci, ri < ci)

    def system(slot, gram, d, rate, col, rowv):
        spread = jnp.where(strict[d], col - rowv, 0.0)
        s = jnp.where(strict[d], gram * (-rate) * jnp.exp(spread), 0.0)
        low[slot] = s.astype(BF16)
        inv[slot] = (eye + jnp.where(apart == 1, s, 0.0)).astype(BF16)

    half = BLOCK // 2
    same = apart < half
    crate = jnp.concatenate([rates[lats:]] * 2, axis=0)
    clog = jnp.concatenate([logs[lats:]] * 2, axis=0)
    cfwd = exact_dot(jnp.where(same, lower, 0.0), clog)
    cbwd = exact_dot(jnp.where(same, upper, 0.0), clog)
    first = lax.broadcasted_iota(jnp.int32, (BLOCK, 1), 0) < half
    cr = [jnp.where(first, crate[:, 2 * d : 2 * d + 1], crate[:, 2 * d + 1 : 2 * d + 2]) for d in (0, 1)]
    cg = [
        jnp.where(first, c[:, 4 + 2 * d : 5 + 2 * d], c[:, 5 + 2 * d : 6 + 2 * d])
        for d, c in ((0, cfwd), (1, cbwd))
    ]
    cgt = jnp.where(ci == 0, cg[0], cg[1]).T
    ck = [unit(k_ref[lats:, h * HEAD_DIM : (h + 1) * HEAD_DIM]) for h in (0, 1)]
    ckk = jnp.concatenate(ck, axis=0)
    cvv = jnp.concatenate(
        [v_ref[lats:, h * HEAD_DIM : (h + 1) * HEAD_DIM].astype(F32) for h in (0, 1)], axis=0
    )
    ckb = ckk.astype(BF16)
    cgram = jnp.where(same, dot_t(ckb, ckb), 0.0)
    for d in (0, 1):
        system(4 * nblk + d, cgram, d, cr[d], cg[d], cgt[d : d + 1])

    keys = [[None] * nblk for _ in (0, 1)]
    for b in range(nblk):
        rows = slice(b * BLOCK, (b + 1) * BLOCK)
        fwd = exact_dot(lower, logs[rows])
        bwd = exact_dot(upper, logs[rows])
        both = jnp.where(ci < 4, rates[rows], jnp.where(ci < 6, fwd, bwd))
        turned = both.T
        gates_ref[b, 0] = both
        gates_ref[b, 1] = turned
        for h in (0, 1):
            kk = unit(k_ref[rows, h * HEAD_DIM : (h + 1) * HEAD_DIM])
            kb = kk.astype(BF16)
            gram = dot_t(kb, kb)
            for d in (0, 1):
                c = 2 * d + h
                system(c * nblk + b, gram, d, both[:, c : c + 1], both[:, 4 + c : 5 + c], turned[4 + c : 5 + c])

    count = 4 * nblk + 2

    def level(i, size):
        pick = (apart >= size) & (apart < 2 * size)
        halves = []
        for s in range(count):
            t = inv[s]
            m = jnp.where(pick, low[s], jnp.zeros((), BF16))
            halves.append(dot(t, m).astype(BF16))
        for s in range(count):
            t = inv[s]
            inv[s] = t + dot(halves[s], t).astype(BF16)
        return size * 2

    lax.fori_loop(0, 6, level, jnp.int32(2))

    for d in (0, 1):
        side = jnp.concatenate([cvv * cr[d], ckk * (cr[d] * jnp.exp(cg[d]))], axis=1)
        solved = dot(inv[4 * nblk + d], side.astype(BF16))
        packed = jnp.concatenate([-solved[:, HEAD_DIM:], solved[:, :HEAD_DIM]], axis=1).astype(BF16)
        for h in (0, 1):
            c = 2 * d + h
            rows = slice(h * half, (h + 1) * half)
            end = (h * half + half - 1) if d == 0 else h * half
            last = cg[d][end : end + 1]
            late = ckk[rows] * jnp.exp(last - cg[d][rows])
            ab = t_dot(late.astype(BF16), packed[rows])
            change = (ab[:, :HEAD_DIM] + eye * (jnp.exp(last) - 1.0)).astype(BF16)
            add = ab[:, HEAD_DIM:].T.astype(BF16)
            for s in range(4):
                send_ref[s * 4 + c, BLOCK : 2 * BLOCK] = change
                send_ref[s * 4 + c, 2 * BLOCK + SLICE :] = add[s * SLICE : (s + 1) * SLICE]

    for b in range(nblk):
        rows = slice(b * BLOCK, (b + 1) * BLOCK)
        both = gates_ref[b, 0]
        for h in (0, 1):
            cols = slice(h * HEAD_DIM, (h + 1) * HEAD_DIM)
            kk = unit(k_ref[rows, cols])
            vv = v_ref[rows, cols].astype(F32)
            for d in (0, 1):
                c = 2 * d + h
                rate = both[:, c : c + 1]
                g = both[:, 4 + c : 5 + c]
                side = jnp.concatenate([kk * (rate * jnp.exp(g)), vv * rate], axis=1).astype(BF16)
                uw[c * nblk + b] = dot(inv[c * nblk + b], side)

    start = jnp.concatenate([eye, jnp.zeros_like(eye)], axis=1)
    states = [start] * 4
    for t in range(nblk):
        for c in range(4):
            d, h = c // 2, c % 2
            b = t if d == 0 else nblk - 1 - t
            rows = slice(b * BLOCK, (b + 1) * BLOCK)
            state = states[c]
            sb = state.astype(BF16)
            sv_ref[c * nblk + b, :BLOCK] = sb
            solved = uw[c * nblk + b]
            moved = dot(solved[:, :HEAD_DIM].astype(BF16), sb)
            fresh = jnp.concatenate(
                [-moved[:, :HEAD_DIM], solved[:, HEAD_DIM:] - moved[:, HEAD_DIM:]], axis=1
            ).astype(BF16)
            sv_ref[c * nblk + b, BLOCK:] = fresh
            g = gates_ref[b, 0][:, 4 + c : 5 + c]
            end = BLOCK - 1 if d == 0 else 0
            last = g[end : end + 1]
            kk = unit(k_ref[rows, h * HEAD_DIM : (h + 1) * HEAD_DIM])
            late = (kk * jnp.exp(last - g)).astype(BF16)
            states[c] = state * jnp.exp(last) + t_dot(late, fresh)
    for c in range(4):
        change = (states[c][:, :HEAD_DIM] - eye).astype(BF16)
        add = states[c][:, HEAD_DIM:].T.astype(BF16)
        for s in range(4):
            send_ref[s * 4 + c, :BLOCK] = change
            send_ref[s * 4 + c, 2 * BLOCK : 2 * BLOCK + SLICE] = add[s * SLICE : (s + 1) * SLICE]


def chunk_maps(k, v, g, bias, log_rate):
    nblk = (k.shape[0] - 64) // BLOCK
    count = 4 * nblk
    return pl.pallas_call(
        maps_kernel,
        out_shape=[
            jax.ShapeDtypeStruct((16, 2 * BLOCK + 2 * SLICE, HEAD_DIM), BF16),
            jax.ShapeDtypeStruct((count, 2 * BLOCK, 2 * HEAD_DIM), BF16),
            jax.ShapeDtypeStruct((nblk, 2, BLOCK, 128), F32),
        ],
        scratch_shapes=[
            pltpu.VMEM((count + 2, BLOCK, BLOCK), BF16),
            pltpu.VMEM((count + 2, BLOCK, BLOCK), BF16),
            pltpu.VMEM((count, BLOCK, 2 * HEAD_DIM), F32),
        ],
        name="chunk_maps",
    )(k, v, g, bias, log_rate)


def query_kernel(q_ref, k_ref, sv_ref, gates_ref, eff_ref, local_ref):
    nblk = q_ref.shape[0] // BLOCK
    ri, ci = iotas(BLOCK)
    seen = (ri >= ci, ri <= ci)
    for b in range(nblk):
        rows = slice(b * BLOCK, (b + 1) * BLOCK)
        both = gates_ref[b, 0]
        turned = gates_ref[b, 1]
        for h in (0, 1):
            cols = slice(h * HEAD_DIM, (h + 1) * HEAD_DIM)
            qq = unit(q_ref[rows, cols]) * HEAD_DIM**-0.5
            kb = unit(k_ref[rows, cols]).astype(BF16)
            scores = dot_t(qq.astype(BF16), kb)
            local = None
            for d in (0, 1):
                c = 2 * d + h
                g = both[:, 4 + c : 5 + c]
                spread = jnp.where(seen[d], g - turned[4 + c : 5 + c], 0.0)
                decayed = jnp.where(seen[d], scores * jnp.exp(spread), 0.0)
                side = jnp.concatenate([qq * jnp.exp(g), decayed], axis=1).astype(BF16)
                out = dot(side, sv_ref[c * nblk + b])
                eff_ref[h, rows, d * HEAD_DIM : (d + 1) * HEAD_DIM] = out[:, :HEAD_DIM].astype(BF16)
                local = out[:, HEAD_DIM:] if local is None else local + out[:, HEAD_DIM:]
            local_ref[h, rows] = local


def query_parts(q, k, sv, gates):
    rows = q.shape[0]
    return pl.pallas_call(
        query_kernel,
        out_shape=[
            jax.ShapeDtypeStruct((2, rows, 2 * HEAD_DIM), BF16),
            jax.ShapeDtypeStruct((2, rows, HEAD_DIM), F32),
        ],
        name="query_parts",
    )(q, k, sv, gates)


def states_kernel(back_ref, recv_ref, out_ref):
    back = back_ref[0]
    peers = recv_ref.shape[0]

    def at(t):
        return jnp.where(back == 1, peers - 1 - t, t)

    def advance(state, change, add):
        hi = state.astype(BF16)
        lo = (state - hi.astype(F32)).astype(BF16)
        moved = dot_t(jnp.concatenate([hi, lo], axis=0), change)
        return state + moved[:SLICE] + moved[SLICE:] + add.astype(F32)

    state = recv_ref[at(0), 2 * BLOCK + SLICE :].astype(F32)
    for t in range(1, peers):
        i = at(t)
        state = advance(state, recv_ref[i, BLOCK : 2 * BLOCK], recv_ref[i, 2 * BLOCK + SLICE :])
    for t in range(peers):
        i = at(t)
        out_ref[i] = state.astype(BF16)
        if t < peers - 1:
            state = advance(state, recv_ref[i, :BLOCK], recv_ref[i, 2 * BLOCK : 2 * BLOCK + SLICE])


def entering_states(back, recv):
    peers = recv.shape[0]
    return pl.pallas_call(
        states_kernel,
        in_specs=[
            pl.BlockSpec(memory_space=pltpu.SMEM),
            pl.BlockSpec(memory_space=pltpu.VMEM),
        ],
        out_shape=jax.ShapeDtypeStruct((peers, SLICE, HEAD_DIM), BF16),
        name="entering_states",
    )(back, recv)


def heads_kernel(states_ref, eff_ref, local_ref, gain_ref, out_ref):
    for h in (0, 1):
        turned = [
            jnp.concatenate([states_ref[s * 4 + 2 * d + h] for s in range(4)], axis=0) for d in (0, 1)
        ]
        combined = local_ref[h] + dot_t(eff_ref[h], jnp.concatenate(turned, axis=1))
        scale = lax.rsqrt(jnp.mean(combined * combined, axis=-1, keepdims=True) + EPS)
        out_ref[:, h * HEAD_DIM : (h + 1) * HEAD_DIM] = (combined * scale * gain_ref[...]).astype(BF16)


def head_outputs(states, eff, local, gain):
    rows = eff.shape[1]
    return pl.pallas_call(
        heads_kernel,
        out_shape=jax.ShapeDtypeStruct((rows, 2 * HEAD_DIM), BF16),
        name="head_outputs",
    )(states, eff, local, gain)


def update_kernel(place_ref, mine_ref, other_ref, w_ref, lat_ref, gate_ref, out_ref):
    y, core = place_ref[0], place_ref[1]
    n = mine_ref.shape[2]
    acc = None
    for ref, which in ((mine_ref, core), (other_ref, 1 - core)):
        for i, off in enumerate((0, 3, 1, 2)):
            peer = lax.rem(y + off, 4) * 2 + which
            part = dot(ref[i], w_ref[pl.ds(pl.multiple_of(peer * n, n), n), :])
            acc = part if acc is None else acc + part
    out_ref[...] = (lat_ref[...].astype(F32) + gate_ref[...] * acc).astype(BF16)


def update(place, mine, other, w, latent, gate):
    rows = latent.shape[0]
    ncol = w.shape[1]
    grid = pltpu.PrefetchScalarGridSpec(
        num_scalar_prefetch=1,
        grid=(1,),
        in_specs=[
            pl.BlockSpec(mine.shape, lambda i, p: (0, 0, 0)),
            pl.BlockSpec(other.shape, lambda i, p: (0, 0, 0)),
            pl.BlockSpec(w.shape, lambda i, p: (0, 0)),
            pl.BlockSpec((rows, ncol), lambda i, p: (0, p[0] * 2 + p[1])),
            pl.BlockSpec((1, ncol), lambda i, p: (0, 0)),
        ],
        out_specs=pl.BlockSpec((rows, ncol), lambda i, p: (0, 0)),
    )
    return pl.pallas_call(
        update_kernel,
        grid_spec=grid,
        out_shape=jax.ShapeDtypeStruct((rows, ncol), BF16),
        name="update",
    )(place, mine, other, w, latent, gate)


def body(
    latent,
    context,
    condition,
    context_condition,
    shift_weight,
    scale_weight,
    gate_weight,
    norm_gain,
    query_weight,
    key_weight,
    value_weight,
    write_weight,
    decay_weight,
    write_bias,
    decay_bias,
    log_rate,
    head_gain,
    out_weight,
):
    heads = query_weight.shape[1] // HEAD_DIM
    y, core = lax.axis_index("y"), lax.axis_index("c")
    part = y * 2 + core
    first_head = part * heads
    parts = lax.axis_size(TP)
    peers = lax.axis_size(SP)

    stacked = jnp.stack([condition, context_condition]).astype(F32)
    silu_rows = jax.nn.silu(stacked).astype(BF16)
    rows5 = jnp.concatenate(
        [dot(silu_rows, shift_weight), dot(silu_rows, scale_weight), dot(silu_rows[:1], gate_weight)]
    ).astype(BF16)
    copies = jnp.broadcast_to(rows5, (peers * parts, *rows5.shape))
    recv = lax.all_to_all(copies, ALL, split_axis=0, concat_axis=0, tiled=True)
    recv = recv.reshape(peers, parts, *rows5.shape)
    gate_row = jnp.sum(
        lax.dynamic_index_in_dim(recv[:, :, 4], part, 1, keepdims=False).astype(F32), axis=0, keepdims=True
    )

    def own(a):
        return lax.dynamic_slice_in_dim(a, first_head, heads, a.ndim - 1)

    gates_w = jnp.concatenate(
        [own(write_weight).reshape(-1, 2 * heads), own(decay_weight).reshape(-1, 2 * heads)], axis=1
    )
    gates_w = jnp.pad(gates_w, ((0, 0), (0, 128 - gates_w.shape[1])))

    def lanes(*pieces):
        r = jnp.concatenate([p.reshape(1, -1) for p in pieces], axis=1)
        return jnp.pad(r, ((0, 0), (0, 128 - r.shape[1])))

    bias = lanes(own(write_bias), own(decay_bias))
    logs = lanes(jnp.zeros((2, heads), F32), own(log_rate))

    ls, cs = row_scales(latent, context)
    q, k, v, g = projections(
        recv,
        norm_gain.reshape(1, -1),
        latent,
        context,
        ls,
        cs,
        query_weight,
        key_weight,
        value_weight,
        gates_w,
    )
    send, sv, gates = chunk_maps(k, v, g, bias, logs)
    maps = lax.all_to_all(send, SP, split_axis=0, concat_axis=0, tiled=True)
    eff, local = query_parts(q, k, sv, gates)
    chain = lax.rem(lax.axis_index("x"), 4)
    back = (chain // 2).astype(jnp.int32).reshape(1)
    starts = entering_states(back, maps)
    states = lax.all_to_all(starts, SP, split_axis=0, concat_axis=0, tiled=True)
    head_out = head_outputs(states, eff, local, head_gain.reshape(1, -1))

    n = lax.axis_size("y")
    up = [(i, (i + 1) % n) for i in range(n)]
    down = [(i, (i - 1) % n) for i in range(n)]
    cut = head_out.shape[0] // 2
    below = lax.ppermute(head_out, "y", up)
    above = lax.ppermute(head_out, "y", down)
    far_a = lax.ppermute(below[:cut], "y", up)
    far_b = lax.ppermute(above[cut:], "y", down)
    mine = jnp.stack([head_out, below, above, jnp.concatenate([far_a, far_b])])
    other = lax.ppermute(mine, "c", [(0, 1), (1, 0)])
    place = jnp.stack([y, core]).astype(jnp.int32)
    return update(place, mine, other, out_weight, latent, gate_row)


def solution(mesh):
    torus = Mesh(mesh.devices.reshape(4, 4, 4, 2), ALL)
    placed = (
        P(SP, None),
        P(SP, None),
        P(SP),
        P(SP),
        P(SP, TP),
        P(SP, TP),
        P(SP, TP),
        P(),
        P(None, TP),
        P(None, TP),
        P(None, TP),
        P(),
        P(),
        P(),
        P(),
        P(),
        P(),
        P(None, TP),
    )
    return jax.shard_map(body, mesh=torus, in_specs=placed, out_specs=P(SP, TP), check_vma=False)
```

```python
import functools

import jax
import jax.numpy as jnp
from jax import lax
from jax.experimental import pallas as pl
from jax.experimental.pallas import tpu as pltpu
from jax.sharding import Mesh
from jax.sharding import PartitionSpec as P

HEAD_DIM = 128
BLOCK = 128
SP = ("z", "x")
TP = ("y", "c")
ALL = ("z", "x", "y", "c")
SLICE = 32
EPS = 0.0001
F32 = jnp.float32
BF16 = jnp.bfloat16


def dot(a, b):
    return jnp.dot(a, b, preferred_element_type=F32)


def dot_t(a, b):
    return lax.dot_general(a, b, (((1,), (1,)), ((), ())), preferred_element_type=F32)


def t_dot(a, b):
    return lax.dot_general(a, b, (((0,), (0,)), ((), ())), preferred_element_type=F32)


def running_sums(mask, x):
    hi = x.astype(BF16)
    rest = x - hi.astype(F32)
    mid = rest.astype(BF16)
    low = (rest - mid.astype(F32)).astype(BF16)
    n = x.shape[1]
    out = dot(mask, jnp.concatenate([hi, mid, low], axis=1))
    return out[:, :n] + out[:, n : 2 * n] + out[:, 2 * n :]


def iotas(n):
    shape = (n, n)
    return lax.broadcasted_iota(jnp.int32, shape, 0), lax.broadcasted_iota(jnp.int32, shape, 1)


def unit(x):
    x = x.astype(F32)
    return x * lax.rsqrt(jnp.sum(x * x, axis=-1, keepdims=True) + EPS)


def log1p_small(e):
    series = e * (1.0 - e * (0.5 - e * (1.0 / 3.0 - 0.25 * e)))
    return jnp.where(e < 0.01, series, jnp.log(1.0 + e))


def softplus(x):
    return jnp.maximum(x, 0.0) + log1p_small(jnp.exp(-jnp.abs(x)))


VMEM = pl.BlockSpec(memory_space=pltpu.VMEM)
PIECES = 4


def limit(mib):
    return pltpu.CompilerParams(vmem_limit_bytes=mib * 1024 * 1024)


HBM = pl.BlockSpec(memory_space=pltpu.HBM)


def fetches(pairs, sems):
    copies = [pltpu.make_async_copy(src, dst, sems.at[i]) for i, (src, dst) in enumerate(pairs)]
    for c in copies:
        c.start()
    return copies


def partial_sums_kernel(
    cond_ref, ctx_cond_ref, shift_ref, scale_ref, gate_ref, out_ref, gate_out, w_shift, w_scale, w_gate, sems
):
    copies = fetches(((shift_ref, w_shift), (scale_ref, w_scale), (gate_ref, w_gate)), sems)
    n = cond_ref.shape[0]
    u = jnp.concatenate([r[...].astype(F32).reshape(1, n) for r in (cond_ref, ctx_cond_ref)] * 4, axis=0)
    s = (u * jax.nn.sigmoid(u)).astype(BF16)
    every = []
    for copy, w in zip(copies[:2], (w_shift, w_scale)):
        copy.wait()
        sums = dot(s, w[...])
        every += [sums[0:1], sums[1:2]]
    pieces = [r[:, p * 128 : (p + 1) * 128] for r in every for p in range(PIECES)]
    block = jnp.concatenate(pieces, axis=0).astype(BF16)
    for j in range(out_ref.shape[0]):
        out_ref[j] = block
    copies[2].wait()
    gate = dot(s, w_gate[...])[0:1]
    gate = jnp.concatenate([gate[:, p * 128 : (p + 1) * 128] for p in range(PIECES)], axis=0)
    hi = gate.astype(BF16)
    gate_out[...] = jnp.concatenate([hi, (gate - hi.astype(F32)).astype(BF16)], axis=0)


def partial_sums(cond, ctx_cond, shift, scale, gate, peers):
    return pl.pallas_call(
        partial_sums_kernel,
        in_specs=[VMEM] * 2 + [HBM] * 3,
        out_specs=[VMEM] * 2,
        out_shape=[
            jax.ShapeDtypeStruct((peers, 4 * PIECES, 128), BF16),
            jax.ShapeDtypeStruct((2 * PIECES, 128), BF16),
        ],
        scratch_shapes=[pltpu.VMEM(shift.shape, BF16)] * 3 + [pltpu.SemaphoreType.DMA((3,))],
        compiler_params=limit(60),
        name="partial_sums",
    )(cond, ctx_cond, shift, scale, gate)


def row_scale_kernel(lat_ref, ctx_ref, lat_out, ctx_out):
    def scale(ref):
        x = ref[...].astype(F32)
        s = lax.rsqrt(jnp.mean(x * x, axis=-1, keepdims=True) + EPS)
        return jnp.broadcast_to(s, (x.shape[0], 128))

    lat_out[...] = scale(lat_ref)

    @pl.when(pl.program_id(0) == 0)
    def _():
        ctx_out[...] = scale(ctx_ref)


def row_scales(latent, context):
    rows, width = latent.shape
    crows = context.shape[0]
    step = 128
    return pl.pallas_call(
        row_scale_kernel,
        grid=(rows // step,),
        in_specs=[
            pl.BlockSpec((step, width), lambda i: (i, 0)),
            pl.BlockSpec((crows, width), lambda i: (0, 0)),
        ],
        out_specs=[
            pl.BlockSpec((step, 128), lambda i: (i, 0)),
            pl.BlockSpec((crows, 128), lambda i: (0, 0)),
        ],
        out_shape=[
            jax.ShapeDtypeStruct((rows, 128), F32),
            jax.ShapeDtypeStruct((crows, 128), F32),
        ],
        compiler_params=limit(8),
        name="row_scales",
    )(latent, context)


def modulate(i, mods_ref, gain_ref, pieces, m_ref):
    for p in range(PIECES):
        f = i * PIECES + p
        cols = pl.ds(pl.multiple_of(f * 128, 128), 128)
        gain = gain_ref[pl.ds(f, 1)]
        for ref, scale, r, at in pieces:
            n = ref.shape[0]
            shift = mods_ref[i, r * PIECES + p : r * PIECES + p + 1]
            grow = gain * (1.0 + mods_ref[i, (2 + r) * PIECES + p : (2 + r) * PIECES + p + 1])
            x = ref[:, cols].astype(F32)
            m_ref[at : at + n, cols] = (x * scale[...] * grow + shift).astype(BF16)


def project_kernel(
    recv_ref, gain_ref, lat_hbm, ctx_hbm, ls_ref, cs_ref, wk_hbm, wv_hbm, wg_hbm,
    mods_ref, k_out, v_out, g_out, lat_ref, ctx_ref, wk, wv, wg, m_ref, sems,
):
    parts = mods_ref.shape[0]
    rows, width = lat_ref.shape
    step = width // parts
    peers = recv_ref.shape[0] // parts
    cuts = [slice(i * step, (i + 1) * step) for i in range(parts)]
    pairs = [(ctx_hbm, ctx_ref)]
    pairs += [(lat_hbm.at[:, c], lat_ref.at[:, c]) for c in cuts]
    pairs += [(wk_hbm, wk), (wv_hbm, wv), (wg_hbm, wg)]
    copies = fetches(pairs, sems)
    for t in range(parts):
        total = recv_ref[t].astype(F32)
        for j in range(1, peers):
            total = total + recv_ref[j * parts + t].astype(F32)
        mods_ref[t] = total
    copies[0].wait()
    for i in range(parts):
        copies[1 + i].wait()
        modulate(i, mods_ref, gain_ref, ((lat_ref, ls_ref, 0, 0), (ctx_ref, cs_ref, 1, rows)), m_ref)
    for copy, w, o in zip(copies[1 + parts :], (wk, wv, wg), (k_out, v_out, g_out)):
        copy.wait()
        o[...] = dot(m_ref[...], w[...]).astype(BF16)


def projections(recv, gain, latent, context, ls, cs, wk, wv, wg, parts):
    rows, width = latent.shape
    every = rows + context.shape[0]
    ncol = wk.shape[1]
    gcol = wg.shape[1]
    return pl.pallas_call(
        project_kernel,
        in_specs=[VMEM, VMEM, HBM, HBM, VMEM, VMEM, HBM, HBM, HBM],
        out_specs=[VMEM] * 4,
        out_shape=[
            jax.ShapeDtypeStruct((parts, 4 * PIECES, 128), F32),
            jax.ShapeDtypeStruct((every, ncol), BF16),
            jax.ShapeDtypeStruct((every, ncol), BF16),
            jax.ShapeDtypeStruct((every, gcol), BF16),
        ],
        scratch_shapes=[
            pltpu.VMEM(latent.shape, BF16),
            pltpu.VMEM(context.shape, BF16),
            pltpu.VMEM(wk.shape, BF16),
            pltpu.VMEM(wv.shape, BF16),
            pltpu.VMEM(wg.shape, BF16),
            pltpu.VMEM((every, width), BF16),
            pltpu.SemaphoreType.DMA((parts + 4,)),
        ],
        compiler_params=limit(60),
        name="projections",
    )(recv, gain, latent, context, ls, cs, wk, wv, wg)


def maps_kernel(
    k_ref, v_ref, g_ref, bias_ref, log_rate_ref, part_ref, send_hbm, sv_hbm, gates_hbm,
    send_ref, sv_ref, gates_ref, low, inv, uw, kn, sems, sv_sems,
):
    nblk = (k_ref.shape[0] - 64) // BLOCK
    lats = nblk * BLOCK
    for j in range(send_ref.shape[0]):
        send_ref[j, 2 * BLOCK + 2 * SLICE :] = part_ref[...]
    ri, ci = iotas(BLOCK)
    apart = ri ^ ci
    eye = (ri == ci).astype(F32)
    pre = g_ref[...].astype(F32) + bias_ref[...]
    rates = jax.nn.sigmoid(pre)
    logs = -jnp.exp(log_rate_ref[...]) * softplus(pre)
    below = ri >= ci
    for h in (0, 1):
        kn[h] = unit(k_ref[:, h * HEAD_DIM : (h + 1) * HEAD_DIM])
    strict = (ri > ci, ri < ci)

    def system(slot, gram, d, rate, col, rowv):
        spread = jnp.where(strict[d], col - rowv, 0.0)
        s = jnp.where(strict[d], gram * (-rate) * jnp.exp(spread), 0.0)
        low[slot] = s.astype(BF16)
        inv[slot] = (eye + jnp.where(apart == 1, s, 0.0)).astype(BF16)

    half = BLOCK // 2
    same = apart < half
    crate = jnp.concatenate([rates[lats:]] * 2, axis=0)
    clog = jnp.concatenate([logs[lats:]] * 2, axis=0)
    cfwd = running_sums((below & same).astype(BF16), clog)
    top = lax.broadcasted_iota(jnp.int32, (BLOCK, 1), 0) < half
    cbwd = clog - cfwd + jnp.where(top, cfwd[half - 1 : half], cfwd[BLOCK - 1 :])
    cr = [jnp.where(top, crate[:, 2 * d : 2 * d + 1], crate[:, 2 * d + 1 : 2 * d + 2]) for d in (0, 1)]
    cg = [
        jnp.where(top, c[:, 4 + 2 * d : 5 + 2 * d], c[:, 5 + 2 * d : 6 + 2 * d])
        for d, c in ((0, cfwd), (1, cbwd))
    ]
    cgt = jnp.where(ci == 0, cg[0], cg[1]).T
    ck = [kn[h, lats:] for h in (0, 1)]
    ckk = jnp.concatenate(ck, axis=0)
    cvv = jnp.concatenate(
        [v_ref[lats:, h * HEAD_DIM : (h + 1) * HEAD_DIM].astype(F32) for h in (0, 1)], axis=0
    )
    ckb = ckk.astype(BF16)
    cgram = jnp.where(same, dot_t(ckb, ckb), 0.0)
    for d in (0, 1):
        system(4 * nblk + d, cgram, d, cr[d], cg[d], cgt[d : d + 1])

    keys = [[None] * nblk for _ in (0, 1)]
    for b in range(nblk):
        rows = slice(b * BLOCK, (b + 1) * BLOCK)
        fwd = running_sums(below.astype(BF16), logs[rows])
        bwd = logs[rows] - fwd + fwd[BLOCK - 1 :]
        both = jnp.where(ci < 4, rates[rows], jnp.where(ci < 6, fwd, bwd))
        turned = both.T
        gates_ref[b, 0] = both
        gates_ref[b, 1] = turned
        for h in (0, 1):
            kb = kn[h, rows].astype(BF16)
            gram = dot_t(kb, kb)
            for d in (0, 1):
                c = 2 * d + h
                system(c * nblk + b, gram, d, both[:, c : c + 1], both[:, 4 + c : 5 + c], turned[4 + c : 5 + c])

    count = 4 * nblk + 2

    def level(i, size):
        pick = (apart >= size) & (apart < 2 * size)
        halves = []
        for s in range(count):
            t = inv[s]
            m = jnp.where(pick, low[s], jnp.zeros((), BF16))
            halves.append(dot(t, m).astype(BF16))
        for s in range(count):
            t = inv[s]
            inv[s] = t + dot(halves[s], t).astype(BF16)
        return size * 2

    lax.fori_loop(0, 6, level, jnp.int32(2))

    for d in (0, 1):
        side = jnp.concatenate([cvv * cr[d], ckk * (cr[d] * jnp.exp(cg[d]))], axis=1)
        solved = dot(inv[4 * nblk + d], side.astype(BF16))
        packed = jnp.concatenate([-solved[:, HEAD_DIM:], solved[:, :HEAD_DIM]], axis=1).astype(BF16)
        for h in (0, 1):
            c = 2 * d + h
            rows = slice(h * half, (h + 1) * half)
            end = (h * half + half - 1) if d == 0 else h * half
            last = cg[d][end : end + 1]
            late = ckk[rows] * jnp.exp(last - cg[d][rows])
            ab = t_dot(late.astype(BF16), packed[rows])
            change = (ab[:, :HEAD_DIM] + eye * (jnp.exp(last) - 1.0)).astype(BF16)
            add = ab[:, HEAD_DIM:].T.astype(BF16)
            for s in range(4):
                send_ref[s * 4 + c, BLOCK : 2 * BLOCK] = change
                send_ref[s * 4 + c, 2 * BLOCK + SLICE : 2 * BLOCK + 2 * SLICE] = add[s * SLICE : (s + 1) * SLICE]

    lat_rows = (slice(0, BLOCK), slice(2 * BLOCK, 2 * BLOCK + SLICE))
    ctx_rows = (slice(BLOCK, 2 * BLOCK), slice(2 * BLOCK + SLICE, send_ref.shape[1]))
    pairs = [(gates_ref, gates_hbm)] + [(send_ref.at[:, r], send_hbm.at[:, r]) for r in ctx_rows]
    waiting = fetches(pairs, sems)

    for b in range(nblk):
        rows = slice(b * BLOCK, (b + 1) * BLOCK)
        both = gates_ref[b, 0]
        for h in (0, 1):
            cols = slice(h * HEAD_DIM, (h + 1) * HEAD_DIM)
            kk = kn[h, rows]
            vv = v_ref[rows, cols].astype(F32)
            for d in (0, 1):
                c = 2 * d + h
                rate = both[:, c : c + 1]
                g = both[:, 4 + c : 5 + c]
                side = jnp.concatenate([kk * (rate * jnp.exp(g)), vv * rate], axis=1).astype(BF16)
                uw[c * nblk + b] = dot(inv[c * nblk + b], side)

    start = jnp.concatenate([eye, jnp.zeros_like(eye)], axis=1)
    states = [start] * 4
    for t in range(nblk):
        for c in range(4):
            d, h = c // 2, c % 2
            b = t if d == 0 else nblk - 1 - t
            rows = slice(b * BLOCK, (b + 1) * BLOCK)
            state = states[c]
            sb = state.astype(BF16)
            sv_ref[c * nblk + b, :BLOCK] = sb
            solved = uw[c * nblk + b]
            moved = dot(solved[:, :HEAD_DIM].astype(BF16), sb)
            fresh = jnp.concatenate(
                [-moved[:, :HEAD_DIM], solved[:, HEAD_DIM:] - moved[:, HEAD_DIM:]], axis=1
            ).astype(BF16)
            sv_ref[c * nblk + b, BLOCK:] = fresh
            g = gates_ref[b, 0][:, 4 + c : 5 + c]
            end = BLOCK - 1 if d == 0 else 0
            last = g[end : end + 1]
            late = (kn[h, rows] * jnp.exp(last - g)).astype(BF16)
            states[c] = state * jnp.exp(last) + t_dot(late, fresh)
        for c in range(4):
            b = c * nblk + (t if c < 2 else nblk - 1 - t)
            copy = pltpu.make_async_copy(sv_ref.at[b], sv_hbm.at[b], sv_sems.at[b])
            copy.start()
            waiting.append(copy)
    for c in range(4):
        change = (states[c][:, :HEAD_DIM] - eye).astype(BF16)
        add = states[c][:, HEAD_DIM:].T.astype(BF16)
        for s in range(4):
            send_ref[s * 4 + c, :BLOCK] = change
            send_ref[s * 4 + c, 2 * BLOCK : 2 * BLOCK + SLICE] = add[s * SLICE : (s + 1) * SLICE]
    late_pairs = [(send_ref.at[:, r], send_hbm.at[:, r]) for r in lat_rows]
    for i, (src, dst) in enumerate(late_pairs):
        copy = pltpu.make_async_copy(src, dst, sems.at[len(pairs) + i])
        copy.start()
        waiting.append(copy)
    for copy in waiting:
        copy.wait()


def chunk_maps(k, v, g, bias, log_rate, part):
    nblk = (k.shape[0] - 64) // BLOCK
    count = 4 * nblk
    outs = [
        jax.ShapeDtypeStruct((16, 2 * BLOCK + 2 * SLICE + 2 * PIECES, HEAD_DIM), BF16),
        jax.ShapeDtypeStruct((count, 2 * BLOCK, 2 * HEAD_DIM), BF16),
        jax.ShapeDtypeStruct((nblk, 2, BLOCK, 128), F32),
    ]
    return pl.pallas_call(
        maps_kernel,
        in_specs=[VMEM] * 6,
        out_specs=[HBM] * 3,
        out_shape=outs,
        scratch_shapes=[pltpu.VMEM(o.shape, o.dtype) for o in outs]
        + [
            pltpu.VMEM((count + 2, BLOCK, BLOCK), BF16),
            pltpu.VMEM((count + 2, BLOCK, BLOCK), BF16),
            pltpu.VMEM((count, BLOCK, 2 * HEAD_DIM), F32),
            pltpu.VMEM((2, k.shape[0], HEAD_DIM), F32),
            pltpu.SemaphoreType.DMA((5,)),
            pltpu.SemaphoreType.DMA((count,)),
        ],
        compiler_params=limit(60),
        name="chunk_maps",
    )(k, v, g, bias, log_rate, part)


def query_kernel(
    mods_ref, gain_ref, lat_ref, ls_ref, wq_ref, k_ref, sv_ref, gates_ref, eff_ref, local_ref, m_ref, q_ref
):
    nblk = q_ref.shape[0] // BLOCK

    def fill(i, carry):
        modulate(i, mods_ref, gain_ref, ((lat_ref, ls_ref, 0, 0),), m_ref)
        return carry

    lax.fori_loop(0, mods_ref.shape[0], fill, 0)
    q_ref[...] = dot(m_ref[...], wq_ref[...]).astype(BF16)
    ri, ci = iotas(BLOCK)
    seen = (ri >= ci, ri <= ci)
    for b in range(nblk):
        rows = slice(b * BLOCK, (b + 1) * BLOCK)
        both = gates_ref[b, 0]
        turned = gates_ref[b, 1]
        for h in (0, 1):
            cols = slice(h * HEAD_DIM, (h + 1) * HEAD_DIM)
            qq = unit(q_ref[rows, cols]) * HEAD_DIM**-0.5
            kb = unit(k_ref[rows, cols]).astype(BF16)
            scores = dot_t(qq.astype(BF16), kb)
            local = None
            for d in (0, 1):
                c = 2 * d + h
                g = both[:, 4 + c : 5 + c]
                spread = jnp.where(seen[d], g - turned[4 + c : 5 + c], 0.0)
                decayed = jnp.where(seen[d], scores * jnp.exp(spread), 0.0)
                side = jnp.concatenate([qq * jnp.exp(g), decayed], axis=1).astype(BF16)
                out = dot(side, sv_ref[c * nblk + b])
                eff_ref[h, rows, d * HEAD_DIM : (d + 1) * HEAD_DIM] = out[:, :HEAD_DIM].astype(BF16)
                local = out[:, HEAD_DIM:] if local is None else local + out[:, HEAD_DIM:]
            local_ref[h, rows] = local


def query_parts(mods, gain, latent, ls, wq, k, sv, gates):
    rows = latent.shape[0]
    return pl.pallas_call(
        query_kernel,
        in_specs=[VMEM] * 8,
        out_specs=[VMEM] * 2,
        out_shape=[
            jax.ShapeDtypeStruct((2, rows, 2 * HEAD_DIM), BF16),
            jax.ShapeDtypeStruct((2, rows, HEAD_DIM), F32),
        ],
        scratch_shapes=[pltpu.VMEM(latent.shape, BF16), pltpu.VMEM((rows, wq.shape[1]), BF16)],
        compiler_params=limit(60),
        name="query_parts",
    )(mods, gain, latent, ls, wq, k, sv, gates)


GROUP = 4


def states_kernel(back_ref, recv_ref, out_ref, gate_ref, comp):
    back = back_ref[0]
    peers = recv_ref.shape[0]
    gate = recv_ref[0, 2 * BLOCK + 2 * SLICE :].astype(F32)
    for j in range(1, peers):
        gate = gate + recv_ref[j, 2 * BLOCK + 2 * SLICE :].astype(F32)
    gate_ref[...] = gate[:PIECES] + gate[PIECES:]
    groups = peers // GROUP
    ri, ci = iotas(HEAD_DIM)
    eye = (ri == ci).astype(F32)

    def at(t):
        return jnp.where(back == 1, peers - 1 - t, t)

    def through(rows, weight):
        hi = rows.astype(BF16)
        lo = (rows - hi.astype(F32)).astype(BF16)
        n = rows.shape[0]
        moved = dot_t(jnp.concatenate([hi, lo], axis=0), weight)
        return moved[:n] + moved[n:]

    still = jnp.concatenate([eye, jnp.zeros((SLICE, HEAD_DIM), F32)], axis=0)
    running = [[jnp.zeros_like(still)] * groups for _ in (0, 1)]
    for t in range(GROUP):
        for kind in (0, 1):
            base = BLOCK * (1 - kind)
            extra = 2 * BLOCK + SLICE * (1 - kind)
            for g in range(groups):
                i = at(g * GROUP + t)
                rows = running[kind][g]
                moved = through(rows + still, recv_ref[i, base : base + BLOCK])
                add = recv_ref[i, extra : extra + SLICE].astype(F32)
                rows = rows + moved
                rows = jnp.concatenate([rows[:HEAD_DIM], rows[HEAD_DIM:] + add], axis=0)
                running[kind][g] = rows
                if t < GROUP - 1:
                    comp[kind * peers + g * GROUP + t + 1] = rows

    eye16 = eye.astype(BF16)

    def apply(state, rows):
        hi = state.astype(BF16)
        lo = (state - hi.astype(F32)).astype(BF16)
        both = jnp.concatenate([hi, lo], axis=0)
        weight = jnp.concatenate([rows[:HEAD_DIM].astype(BF16), eye16], axis=0)
        moved = dot(jnp.concatenate([both, both], axis=1), weight)
        return moved[:SLICE] + moved[SLICE:] + rows[HEAD_DIM:]

    state = running[0][0][HEAD_DIM:]
    for g in range(1, groups):
        state = apply(state, running[0][g])
    entries = [state]
    for g in range(groups - 1):
        entries.append(apply(entries[-1], running[1][g]))
    for g in range(groups):
        for t in range(GROUP):
            i = at(g * GROUP + t)
            out = entries[g] if t == 0 else apply(entries[g], comp[peers + g * GROUP + t])
            out_ref[i] = out.astype(BF16)


def entering_states(back, recv):
    peers = recv.shape[0]
    return pl.pallas_call(
        states_kernel,
        in_specs=[
            pl.BlockSpec(memory_space=pltpu.SMEM),
            pl.BlockSpec(memory_space=pltpu.VMEM),
        ],
        out_shape=[
            jax.ShapeDtypeStruct((peers, SLICE, HEAD_DIM), BF16),
            jax.ShapeDtypeStruct((PIECES, HEAD_DIM), F32),
        ],
        scratch_shapes=[pltpu.VMEM((2 * peers, HEAD_DIM + SLICE, HEAD_DIM), F32)],
        compiler_params=limit(16),
        name="entering_states",
    )(back, recv)


def heads_kernel(states_ref, eff_hbm, local_hbm, gain_ref, out_ref, eff_ref, local_ref, sems):
    copies = fetches(
        [(src.at[h], dst.at[h]) for h in (0, 1) for src, dst in ((eff_hbm, eff_ref), (local_hbm, local_ref))], sems
    )
    for h in (0, 1):
        turned = [
            jnp.concatenate([states_ref[s * 4 + 2 * d + h] for s in range(4)], axis=0) for d in (0, 1)
        ]
        copies[2 * h].wait()
        copies[2 * h + 1].wait()
        combined = local_ref[h] + dot_t(eff_ref[h], jnp.concatenate(turned, axis=1))
        scale = lax.rsqrt(jnp.mean(combined * combined, axis=-1, keepdims=True) + EPS)
        out_ref[:, h * HEAD_DIM : (h + 1) * HEAD_DIM] = (combined * scale * gain_ref[...]).astype(BF16)


def head_outputs(states, eff, local, gain):
    rows = eff.shape[1]
    return pl.pallas_call(
        heads_kernel,
        in_specs=[VMEM, HBM, HBM, VMEM],
        out_specs=VMEM,
        out_shape=jax.ShapeDtypeStruct((rows, 2 * HEAD_DIM), BF16),
        scratch_shapes=[
            pltpu.VMEM(eff.shape, BF16),
            pltpu.VMEM(local.shape, F32),
            pltpu.SemaphoreType.DMA((4,)),
        ],
        compiler_params=limit(60),
        name="head_outputs",
    )(states, eff, local, gain)


def update_kernel(place_ref, mine_ref, other_ref, w_ref, lat_ref, gate_ref, out_ref):
    y, core = place_ref[0], place_ref[1]
    n = mine_ref.shape[2]
    acc = None
    for ref, which in ((mine_ref, core), (other_ref, 1 - core)):
        for i, off in enumerate((0, 3, 1, 2)):
            peer = lax.rem(y + off, 4) * 2 + which
            part = dot(ref[i], w_ref[pl.ds(pl.multiple_of(peer * n, n), n), :])
            acc = part if acc is None else acc + part
    for p in range(PIECES):
        cols = slice(p * 128, (p + 1) * 128)
        out_ref[:, cols] = (lat_ref[:, cols].astype(F32) + gate_ref[p : p + 1] * acc[:, cols]).astype(BF16)


def update(place, mine, other, w, latent, gate):
    rows = latent.shape[0]
    return pl.pallas_call(
        update_kernel,
        in_specs=[pl.BlockSpec(memory_space=pltpu.SMEM)] + [VMEM] * 5,
        out_specs=VMEM,
        out_shape=jax.ShapeDtypeStruct((rows, w.shape[1]), BF16),
        compiler_params=limit(16),
        name="update",
    )(place, mine, other, w, latent, gate)


def body(
    latent,
    context,
    condition,
    context_condition,
    shift_weight,
    scale_weight,
    gate_weight,
    norm_gain,
    query_weight,
    key_weight,
    value_weight,
    write_weight,
    decay_weight,
    write_bias,
    decay_bias,
    log_rate,
    head_gain,
    out_weight,
):
    heads = query_weight.shape[1] // HEAD_DIM
    y, core = lax.axis_index("y"), lax.axis_index("c")
    part = y * 2 + core
    first_head = part * heads
    parts = lax.axis_size(TP)
    peers = lax.axis_size(SP)

    sums, gate_part = partial_sums(
        condition,
        context_condition,
        shift_weight,
        scale_weight,
        gate_weight,
        peers * parts,
    )
    sums = lax.all_to_all(sums, ALL, split_axis=0, concat_axis=0, tiled=True)

    def own(a):
        return lax.dynamic_slice_in_dim(a, first_head, heads, a.ndim - 1)

    gates_w = jnp.concatenate(
        [own(write_weight).reshape(-1, 2 * heads), own(decay_weight).reshape(-1, 2 * heads)], axis=1
    )
    gates_w = jnp.pad(gates_w, ((0, 0), (0, 128 - gates_w.shape[1])))

    def lanes(*pieces):
        r = jnp.concatenate([p.reshape(1, -1) for p in pieces], axis=1)
        return jnp.pad(r, ((0, 0), (0, 128 - r.shape[1])))

    bias = lanes(own(write_bias), own(decay_bias))
    logs = lanes(jnp.zeros((2, heads), F32), own(log_rate))

    ls, cs = row_scales(latent, context)
    gain = norm_gain.reshape(-1, 128)
    mods, k, v, g = projections(
        sums, gain, latent, context, ls, cs, key_weight, value_weight, gates_w, parts
    )
    send, sv, gates = chunk_maps(k, v, g, bias, logs, gate_part)
    maps = lax.all_to_all(send, SP, split_axis=0, concat_axis=0, tiled=True)
    eff, local = query_parts(mods, gain, latent, ls, query_weight, k, sv, gates)
    maps, eff, local = lax.optimization_barrier((maps, eff, local))
    chain = lax.rem(lax.axis_index("x"), 4)
    back = (chain // 2).astype(jnp.int32).reshape(1)
    starts, gate_row = entering_states(back, maps)
    states = lax.all_to_all(starts, SP, split_axis=0, concat_axis=0, tiled=True)
    head_out = head_outputs(states, eff, local, head_gain.reshape(1, -1))

    n = lax.axis_size("y")
    up = [(i, (i + 1) % n) for i in range(n)]
    down = [(i, (i - 1) % n) for i in range(n)]
    cut = head_out.shape[0] // 2
    below = lax.ppermute(head_out, "y", up)
    above = lax.ppermute(head_out, "y", down)
    far_a = lax.ppermute(below[:cut], "y", up)
    far_b = lax.ppermute(above[cut:], "y", down)
    mine = jnp.stack([head_out, below, above, jnp.concatenate([far_a, far_b])])
    other = lax.ppermute(mine, "c", [(0, 1), (1, 0)])
    place = jnp.stack([y, core]).astype(jnp.int32)
    columns = out_weight.shape[1]
    residual = lax.dynamic_slice_in_dim(latent, part * columns, columns, 1)
    return update(place, mine, other, out_weight, residual, gate_row)


def solution(mesh):
    torus = Mesh(mesh.devices.reshape(4, 4, 4, 2), ALL)
    placed = (
        P(SP, None),
        P(SP, None),
        P(SP),
        P(SP),
        P(SP, TP),
        P(SP, TP),
        P(SP, TP),
        P(),
        P(None, TP),
        P(None, TP),
        P(None, TP),
        P(),
        P(),
        P(),
        P(),
        P(),
        P(),
        P(None, TP),
    )
    return jax.shard_map(body, mesh=torus, in_specs=placed, out_specs=P(SP, TP), check_vma=False)
```

```python
import functools

import jax
import jax.numpy as jnp
from jax import lax
from jax.experimental import pallas as pl
from jax.experimental.pallas import tpu as pltpu
from jax.sharding import Mesh
from jax.sharding import PartitionSpec as P

HEAD_DIM = 128
BLOCK = 128
SP = ("z", "x")
TP = ("y", "c")
ALL = ("z", "x", "y", "c")
SLICE = 32
EPS = 0.0001
F32 = jnp.float32
BF16 = jnp.bfloat16


def dot(a, b):
    return jnp.dot(a, b, preferred_element_type=F32)


def dot_t(a, b):
    return lax.dot_general(a, b, (((1,), (1,)), ((), ())), preferred_element_type=F32)


def t_dot(a, b):
    return lax.dot_general(a, b, (((0,), (0,)), ((), ())), preferred_element_type=F32)


def running_sums(mask, x):
    hi = x.astype(BF16)
    rest = x - hi.astype(F32)
    mid = rest.astype(BF16)
    low = (rest - mid.astype(F32)).astype(BF16)
    n = x.shape[1]
    out = dot(mask, jnp.concatenate([hi, mid, low], axis=1))
    return out[:, :n] + out[:, n : 2 * n] + out[:, 2 * n :]


def iotas(n):
    shape = (n, n)
    return lax.broadcasted_iota(jnp.int32, shape, 0), lax.broadcasted_iota(jnp.int32, shape, 1)


def unit(x):
    x = x.astype(F32)
    return x * lax.rsqrt(jnp.sum(x * x, axis=-1, keepdims=True) + EPS)


def log1p_small(e):
    series = e * (1.0 - e * (0.5 - e * (1.0 / 3.0 - 0.25 * e)))
    return jnp.where(e < 0.01, series, jnp.log(1.0 + e))


def softplus(x):
    return jnp.maximum(x, 0.0) + log1p_small(jnp.exp(-jnp.abs(x)))


VMEM = pl.BlockSpec(memory_space=pltpu.VMEM)
PIECES = 4


def limit(mib):
    return pltpu.CompilerParams(vmem_limit_bytes=mib * 1024 * 1024)


HBM = pl.BlockSpec(memory_space=pltpu.HBM)


def fetches(pairs, sems):
    copies = [pltpu.make_async_copy(src, dst, sems.at[i]) for i, (src, dst) in enumerate(pairs)]
    for c in copies:
        c.start()
    return copies


def partial_sums_kernel(
    cond_hbm, ctx_cond_hbm, shift_ref, scale_ref, gate_ref, out_ref, gate_out,
    cond_ref, ctx_cond_ref, w_shift, w_scale, w_gate, sems,
):
    pairs = ((cond_hbm, cond_ref), (ctx_cond_hbm, ctx_cond_ref))
    copies = fetches(pairs + ((shift_ref, w_shift), (scale_ref, w_scale), (gate_ref, w_gate)), sems)
    copies[0].wait()
    copies[1].wait()
    copies = copies[2:]
    n = cond_ref.shape[0]
    u = jnp.concatenate([r[...].astype(F32).reshape(1, n) for r in (cond_ref, ctx_cond_ref)] * 4, axis=0)
    s = (u * jax.nn.sigmoid(u)).astype(BF16)
    every = []
    for copy, w in zip(copies[:2], (w_shift, w_scale)):
        copy.wait()
        sums = dot(s, w[...])
        every += [sums[0:1], sums[1:2]]
    pieces = [r[:, p * 128 : (p + 1) * 128] for r in every for p in range(PIECES)]
    block = jnp.concatenate(pieces, axis=0).astype(BF16)
    for j in range(out_ref.shape[0]):
        out_ref[j] = block
    copies[2].wait()
    gate = dot(s, w_gate[...])[0:1]
    gate = jnp.concatenate([gate[:, p * 128 : (p + 1) * 128] for p in range(PIECES)], axis=0)
    hi = gate.astype(BF16)
    gate_out[...] = jnp.concatenate([hi, (gate - hi.astype(F32)).astype(BF16)], axis=0)


def partial_sums(cond, ctx_cond, shift, scale, gate, peers):
    return pl.pallas_call(
        partial_sums_kernel,
        in_specs=[HBM] * 5,
        out_specs=[VMEM] * 2,
        out_shape=[
            jax.ShapeDtypeStruct((peers, 4 * PIECES, 128), BF16),
            jax.ShapeDtypeStruct((2 * PIECES, 128), BF16),
        ],
        scratch_shapes=[pltpu.VMEM(cond.shape, BF16)] * 2
        + [pltpu.VMEM(shift.shape, BF16)] * 3
        + [pltpu.SemaphoreType.DMA((5,))],
        compiler_params=limit(60),
        name="partial_sums",
    )(cond, ctx_cond, shift, scale, gate)


def row_scale_kernel(lat_ref, ctx_ref, lat_out, ctx_out):
    def scale(ref):
        x = ref[...].astype(F32)
        s = lax.rsqrt(jnp.mean(x * x, axis=-1, keepdims=True) + EPS)
        return jnp.broadcast_to(s, (x.shape[0], 128))

    lat_out[...] = scale(lat_ref)

    @pl.when(pl.program_id(0) == 0)
    def _():
        ctx_out[...] = scale(ctx_ref)


def row_scales(latent, context):
    rows, width = latent.shape
    crows = context.shape[0]
    step = 128
    return pl.pallas_call(
        row_scale_kernel,
        grid=(rows // step,),
        in_specs=[
            pl.BlockSpec((step, width), lambda i: (i, 0)),
            pl.BlockSpec((crows, width), lambda i: (0, 0)),
        ],
        out_specs=[
            pl.BlockSpec((step, 128), lambda i: (i, 0)),
            pl.BlockSpec((crows, 128), lambda i: (0, 0)),
        ],
        out_shape=[
            jax.ShapeDtypeStruct((rows, 128), F32),
            jax.ShapeDtypeStruct((crows, 128), F32),
        ],
        compiler_params=limit(8),
        name="row_scales",
    )(latent, context)


def modulate(i, mods_ref, gain_ref, pieces, m_ref):
    for p in range(PIECES):
        f = i * PIECES + p
        cols = pl.ds(pl.multiple_of(f * 128, 128), 128)
        gain = gain_ref[pl.ds(f, 1)]
        for ref, scale, r, at in pieces:
            n = ref.shape[0]
            shift = mods_ref[i, r * PIECES + p : r * PIECES + p + 1]
            grow = gain * (1.0 + mods_ref[i, (2 + r) * PIECES + p : (2 + r) * PIECES + p + 1])
            x = ref[:, cols].astype(F32)
            m_ref[at : at + n, cols] = (x * scale[...] * grow + shift).astype(BF16)


def project(recv_ref, gain_ref, ls_ref, cs_ref, queue, small, mods_ref, lat_ref, ctx_ref, m_ref, k_ref, v_ref, g_ref, weights):
    parts = mods_ref.shape[0]
    rows = lat_ref.shape[0]
    peers = recv_ref.shape[0] // parts
    for c in queue:
        c.start()
    for c in queue[:small]:
        c.wait()
    for t in range(parts):
        total = recv_ref[t].astype(F32)
        for j in range(1, peers):
            total = total + recv_ref[j * parts + t].astype(F32)
        mods_ref[t] = total
    for i in range(parts):
        queue[small + i].wait()
        modulate(i, mods_ref, gain_ref, ((lat_ref, ls_ref, 0, 0), (ctx_ref, cs_ref, 1, rows)), m_ref)
    wk, wv, wg = weights
    queue[small + parts].wait()
    k_ref[...] = dot(m_ref[...], wk[...]).astype(BF16)
    queue[small + parts + 1].wait()
    v_ref[...] = dot(m_ref[...], wv[...]).astype(BF16)
    g_ref[...] = dot_t(m_ref[...], wg[...]).astype(BF16)


def maps_kernel(
    recv_hbm, gain_hbm, lat_hbm, ctx_hbm, ls_hbm, cs_hbm, wk_hbm, wv_hbm, wg_hbm, head_ref, wb_ref, db_ref, lr_ref, part_hbm,
    mods_hbm, k_hbm, send_hbm, sv_hbm, gates_hbm,
    recv_ref, gain_ref, lat_ref, ctx_ref, ls_ref, cs_ref, wk, wv, wg, part_ref,
    mods_ref, k_ref, send_ref, sv_ref, gates_ref, m_ref, v_ref, g_ref, low, inv, uw, kn, in_sems, sems, sv_sems,
):
    parts = mods_ref.shape[0]
    step = lat_ref.shape[1] // parts
    cuts = [slice(i * step, (i + 1) * step) for i in range(parts)]
    loads = [(recv_hbm, recv_ref), (gain_hbm, gain_ref), (ls_hbm, ls_ref), (cs_hbm, cs_ref), (ctx_hbm, ctx_ref)]
    loads += [(part_hbm, part_ref), (wg_hbm, wg)]
    small = len(loads)
    loads += [(lat_hbm.at[:, c], lat_ref.at[:, c]) for c in cuts]
    loads += [(wk_hbm, wk), (wv_hbm, wv)]
    queue = [pltpu.make_async_copy(src, dst, in_sems.at[i]) for i, (src, dst) in enumerate(loads)]
    project(
        recv_ref, gain_ref, ls_ref, cs_ref, queue, small, mods_ref, lat_ref, ctx_ref, m_ref, k_ref, v_ref, g_ref, (wk, wv, wg)
    )

    nblk = (k_ref.shape[0] - 64) // BLOCK
    lats = nblk * BLOCK
    lane = lax.broadcasted_iota(jnp.int32, (1, 8), 1)
    bias = jnp.zeros((1, 8), F32)
    speed = jnp.zeros((1, 8), F32)
    for c in range(4):
        d, h = c // 2, head_ref[0] + c % 2
        bias = jnp.where(lane == c, wb_ref[d, h], jnp.where(lane == 4 + c, db_ref[d, h], bias))
        speed = jnp.where(lane == 4 + c, lr_ref[d, h], speed)
    for j in range(send_ref.shape[0]):
        send_ref[j, 2 * BLOCK + 2 * SLICE :] = part_ref[...]
    ri, ci = iotas(BLOCK)
    apart = ri ^ ci
    eye = (ri == ci).astype(F32)
    pre = g_ref[...].astype(F32) + bias
    rates = jax.nn.sigmoid(pre)
    logs = -jnp.exp(speed) * softplus(pre)
    gap = jnp.zeros((pre.shape[0], 120), F32)
    rates = jnp.concatenate([rates, gap], axis=1)
    logs = jnp.concatenate([logs, gap], axis=1)
    below = ri >= ci
    for h in (0, 1):
        kn[h] = unit(k_ref[:, h * HEAD_DIM : (h + 1) * HEAD_DIM])
    strict = (ri > ci, ri < ci)

    def system(slot, gram, d, rate, col, rowv):
        spread = jnp.where(strict[d], col - rowv, 0.0)
        s = jnp.where(strict[d], gram * (-rate) * jnp.exp(spread), 0.0)
        low[slot] = s.astype(BF16)
        inv[slot] = (eye + jnp.where(apart == 1, s, 0.0)).astype(BF16)

    half = BLOCK // 2
    same = apart < half
    crate = jnp.concatenate([rates[lats:]] * 2, axis=0)
    clog = jnp.concatenate([logs[lats:]] * 2, axis=0)
    cfwd = running_sums((below & same).astype(BF16), clog)
    top = lax.broadcasted_iota(jnp.int32, (BLOCK, 1), 0) < half
    cbwd = clog - cfwd + jnp.where(top, cfwd[half - 1 : half], cfwd[BLOCK - 1 :])
    cr = [jnp.where(top, crate[:, 2 * d : 2 * d + 1], crate[:, 2 * d + 1 : 2 * d + 2]) for d in (0, 1)]
    cg = [
        jnp.where(top, c[:, 4 + 2 * d : 5 + 2 * d], c[:, 5 + 2 * d : 6 + 2 * d])
        for d, c in ((0, cfwd), (1, cbwd))
    ]
    cgt = jnp.where(ci == 0, cg[0], cg[1]).T
    ck = [kn[h, lats:] for h in (0, 1)]
    ckk = jnp.concatenate(ck, axis=0)
    cvv = jnp.concatenate(
        [v_ref[lats:, h * HEAD_DIM : (h + 1) * HEAD_DIM].astype(F32) for h in (0, 1)], axis=0
    )
    ckb = ckk.astype(BF16)
    cgram = jnp.where(same, dot_t(ckb, ckb), 0.0)
    for d in (0, 1):
        system(4 * nblk + d, cgram, d, cr[d], cg[d], cgt[d : d + 1])

    keys = [[None] * nblk for _ in (0, 1)]
    for b in range(nblk):
        rows = slice(b * BLOCK, (b + 1) * BLOCK)
        fwd = running_sums(below.astype(BF16), logs[rows])
        bwd = logs[rows] - fwd + fwd[BLOCK - 1 :]
        both = jnp.where(ci < 4, rates[rows], jnp.where(ci < 6, fwd, bwd))
        turned = both.T
        gates_ref[b, 0] = both
        gates_ref[b, 1] = turned
        for h in (0, 1):
            kb = kn[h, rows].astype(BF16)
            gram = dot_t(kb, kb)
            for d in (0, 1):
                c = 2 * d + h
                system(c * nblk + b, gram, d, both[:, c : c + 1], both[:, 4 + c : 5 + c], turned[4 + c : 5 + c])

    count = 4 * nblk + 2

    def level(i, size):
        pick = (apart >= size) & (apart < 2 * size)
        halves = []
        for s in range(count):
            t = inv[s]
            m = jnp.where(pick, low[s], jnp.zeros((), BF16))
            halves.append(dot(t, m).astype(BF16))
        for s in range(count):
            t = inv[s]
            inv[s] = t + dot(halves[s], t).astype(BF16)
        return size * 2

    lax.fori_loop(0, 6, level, jnp.int32(2))

    for d in (0, 1):
        side = jnp.concatenate([cvv * cr[d], ckk * (cr[d] * jnp.exp(cg[d]))], axis=1)
        solved = dot(inv[4 * nblk + d], side.astype(BF16))
        packed = jnp.concatenate([-solved[:, HEAD_DIM:], solved[:, :HEAD_DIM]], axis=1).astype(BF16)
        for h in (0, 1):
            c = 2 * d + h
            rows = slice(h * half, (h + 1) * half)
            end = (h * half + half - 1) if d == 0 else h * half
            last = cg[d][end : end + 1]
            late = ckk[rows] * jnp.exp(last - cg[d][rows])
            ab = t_dot(late.astype(BF16), packed[rows])
            change = (ab[:, :HEAD_DIM] + eye * (jnp.exp(last) - 1.0)).astype(BF16)
            add = ab[:, HEAD_DIM:].T.astype(BF16)
            for s in range(4):
                send_ref[s * 4 + c, BLOCK : 2 * BLOCK] = change
                send_ref[s * 4 + c, 2 * BLOCK + SLICE : 2 * BLOCK + 2 * SLICE] = add[s * SLICE : (s + 1) * SLICE]

    lat_rows = (slice(0, BLOCK), slice(2 * BLOCK, 2 * BLOCK + SLICE))
    ctx_rows = (slice(BLOCK, 2 * BLOCK), slice(2 * BLOCK + SLICE, send_ref.shape[1]))
    pairs = [(gates_ref, gates_hbm), (k_ref, k_hbm), (mods_ref, mods_hbm)] + [(send_ref.at[:, r], send_hbm.at[:, r]) for r in ctx_rows]
    waiting = fetches(pairs, sems)

    for b in range(nblk):
        rows = slice(b * BLOCK, (b + 1) * BLOCK)
        both = gates_ref[b, 0]
        for h in (0, 1):
            cols = slice(h * HEAD_DIM, (h + 1) * HEAD_DIM)
            kk = kn[h, rows]
            vv = v_ref[rows, cols].astype(F32)
            for d in (0, 1):
                c = 2 * d + h
                rate = both[:, c : c + 1]
                g = both[:, 4 + c : 5 + c]
                side = jnp.concatenate([kk * (rate * jnp.exp(g)), vv * rate], axis=1).astype(BF16)
                uw[c * nblk + b] = dot(inv[c * nblk + b], side)

    start = jnp.concatenate([eye, jnp.zeros_like(eye)], axis=1)
    states = [start] * 4
    for t in range(nblk):
        for c in range(4):
            d, h = c // 2, c % 2
            b = t if d == 0 else nblk - 1 - t
            rows = slice(b * BLOCK, (b + 1) * BLOCK)
            state = states[c]
            sb = state.astype(BF16)
            sv_ref[c * nblk + b, :BLOCK] = sb
            solved = uw[c * nblk + b]
            moved = dot(solved[:, :HEAD_DIM].astype(BF16), sb)
            fresh = jnp.concatenate(
                [-moved[:, :HEAD_DIM], solved[:, HEAD_DIM:] - moved[:, HEAD_DIM:]], axis=1
            ).astype(BF16)
            sv_ref[c * nblk + b, BLOCK:] = fresh
            g = gates_ref[b, 0][:, 4 + c : 5 + c]
            end = BLOCK - 1 if d == 0 else 0
            last = g[end : end + 1]
            late = (kn[h, rows] * jnp.exp(last - g)).astype(BF16)
            states[c] = state * jnp.exp(last) + t_dot(late, fresh)
        for c in range(4):
            b = c * nblk + (t if c < 2 else nblk - 1 - t)
            copy = pltpu.make_async_copy(sv_ref.at[b], sv_hbm.at[b], sv_sems.at[b])
            copy.start()
            waiting.append(copy)
    for c in range(4):
        change = (states[c][:, :HEAD_DIM] - eye).astype(BF16)
        add = states[c][:, HEAD_DIM:].T.astype(BF16)
        for s in range(4):
            send_ref[s * 4 + c, :BLOCK] = change
            send_ref[s * 4 + c, 2 * BLOCK : 2 * BLOCK + SLICE] = add[s * SLICE : (s + 1) * SLICE]
    late_pairs = [(send_ref.at[:, r], send_hbm.at[:, r]) for r in lat_rows]
    for i, (src, dst) in enumerate(late_pairs):
        copy = pltpu.make_async_copy(src, dst, sems.at[len(pairs) + i])
        copy.start()
        waiting.append(copy)
    for copy in waiting:
        copy.wait()


def chunk_maps(recv, gain, latent, context, ls, cs, wk, wv, wg, head, wb, db, lr, part, parts):
    rows, width = latent.shape
    every = rows + context.shape[0]
    ncol = wk.shape[1]
    nblk = rows // BLOCK
    count = 4 * nblk
    outs = [
        jax.ShapeDtypeStruct((16, 2 * BLOCK + 2 * SLICE + 2 * PIECES, HEAD_DIM), BF16),
        jax.ShapeDtypeStruct((count, 2 * BLOCK, 2 * HEAD_DIM), BF16),
        jax.ShapeDtypeStruct((nblk, 2, BLOCK, 128), F32),
    ]
    outs = [
        jax.ShapeDtypeStruct((parts, 4 * PIECES, 128), F32),
        jax.ShapeDtypeStruct((every, ncol), BF16),
    ] + outs
    smem = pl.BlockSpec(memory_space=pltpu.SMEM)
    loaded = (recv, gain, latent, context, ls, cs, wk, wv, wg, part)
    return pl.pallas_call(
        maps_kernel,
        in_specs=[HBM] * 9 + [smem] * 4 + [HBM],
        out_specs=[HBM] * 5,
        out_shape=outs,
        scratch_shapes=[pltpu.VMEM(a.shape, a.dtype) for a in loaded]
        + [pltpu.VMEM(o.shape, o.dtype) for o in outs]
        + [
            pltpu.VMEM((every, width), BF16),
            pltpu.VMEM((every, ncol), BF16),
            pltpu.VMEM((every, wg.shape[0]), BF16),
            pltpu.VMEM((count + 2, BLOCK, BLOCK), BF16),
            pltpu.VMEM((count + 2, BLOCK, BLOCK), BF16),
            pltpu.VMEM((count, BLOCK, 2 * HEAD_DIM), F32),
            pltpu.VMEM((2, every, HEAD_DIM), F32),
            pltpu.SemaphoreType.DMA((parts + 9,)),
            pltpu.SemaphoreType.DMA((7,)),
            pltpu.SemaphoreType.DMA((count,)),
        ],
        compiler_params=limit(60),
        name="chunk_maps",
    )(recv, gain, latent, context, ls, cs, wk, wv, wg, head, wb, db, lr, part)


def query_kernel(
    mods_ref, gain_ref, lat_ref, ls_ref, wq_ref, k_ref, sv_ref, gates_ref, eff_ref, local_ref, m_ref, q_ref
):
    nblk = q_ref.shape[0] // BLOCK

    def fill(i, carry):
        modulate(i, mods_ref, gain_ref, ((lat_ref, ls_ref, 0, 0),), m_ref)
        return carry

    lax.fori_loop(0, mods_ref.shape[0], fill, 0)
    q_ref[...] = dot(m_ref[...], wq_ref[...]).astype(BF16)
    ri, ci = iotas(BLOCK)
    seen = (ri >= ci, ri <= ci)
    for b in range(nblk):
        rows = slice(b * BLOCK, (b + 1) * BLOCK)
        both = gates_ref[b, 0]
        turned = gates_ref[b, 1]
        for h in (0, 1):
            cols = slice(h * HEAD_DIM, (h + 1) * HEAD_DIM)
            qq = unit(q_ref[rows, cols]) * HEAD_DIM**-0.5
            kb = unit(k_ref[rows, cols]).astype(BF16)
            scores = dot_t(qq.astype(BF16), kb)
            local = None
            for d in (0, 1):
                c = 2 * d + h
                g = both[:, 4 + c : 5 + c]
                spread = jnp.where(seen[d], g - turned[4 + c : 5 + c], 0.0)
                decayed = jnp.where(seen[d], scores * jnp.exp(spread), 0.0)
                side = jnp.concatenate([qq * jnp.exp(g), decayed], axis=1).astype(BF16)
                out = dot(side, sv_ref[c * nblk + b])
                eff_ref[h, rows, d * HEAD_DIM : (d + 1) * HEAD_DIM] = out[:, :HEAD_DIM].astype(BF16)
                local = out[:, HEAD_DIM:] if local is None else local + out[:, HEAD_DIM:]
            local_ref[h, rows] = local


def query_parts(mods, gain, latent, ls, wq, k, sv, gates):
    rows = latent.shape[0]
    return pl.pallas_call(
        query_kernel,
        in_specs=[VMEM] * 8,
        out_specs=[VMEM] * 2,
        out_shape=[
            jax.ShapeDtypeStruct((2, rows, 2 * HEAD_DIM), BF16),
            jax.ShapeDtypeStruct((2, rows, HEAD_DIM), F32),
        ],
        scratch_shapes=[pltpu.VMEM(latent.shape, BF16), pltpu.VMEM((rows, wq.shape[1]), BF16)],
        compiler_params=limit(60),
        name="query_parts",
    )(mods, gain, latent, ls, wq, k, sv, gates)


GROUP = 4


def states_kernel(back_ref, recv_ref, out_ref, gate_ref, comp):
    back = back_ref[0]
    peers = recv_ref.shape[0]
    gate = recv_ref[0, 2 * BLOCK + 2 * SLICE :].astype(F32)
    for j in range(1, peers):
        gate = gate + recv_ref[j, 2 * BLOCK + 2 * SLICE :].astype(F32)
    gate_ref[...] = gate[:PIECES] + gate[PIECES:]
    groups = peers // GROUP
    ri, ci = iotas(HEAD_DIM)
    eye = (ri == ci).astype(F32)

    def at(t):
        return jnp.where(back == 1, peers - 1 - t, t)

    def through(rows, weight):
        hi = rows.astype(BF16)
        lo = (rows - hi.astype(F32)).astype(BF16)
        n = rows.shape[0]
        moved = dot_t(jnp.concatenate([hi, lo], axis=0), weight)
        return moved[:n] + moved[n:]

    still = jnp.concatenate([eye, jnp.zeros((SLICE, HEAD_DIM), F32)], axis=0)
    running = [[jnp.zeros_like(still)] * groups for _ in (0, 1)]
    for t in range(GROUP):
        for kind in (0, 1):
            base = BLOCK * (1 - kind)
            extra = 2 * BLOCK + SLICE * (1 - kind)
            for g in range(groups):
                i = at(g * GROUP + t)
                rows = running[kind][g]
                moved = through(rows + still, recv_ref[i, base : base + BLOCK])
                add = recv_ref[i, extra : extra + SLICE].astype(F32)
                rows = rows + moved
                rows = jnp.concatenate([rows[:HEAD_DIM], rows[HEAD_DIM:] + add], axis=0)
                running[kind][g] = rows
                if t < GROUP - 1:
                    comp[kind * peers + g * GROUP + t + 1] = rows

    eye16 = eye.astype(BF16)

    def apply(state, rows):
        hi = state.astype(BF16)
        lo = (state - hi.astype(F32)).astype(BF16)
        both = jnp.concatenate([hi, lo], axis=0)
        weight = jnp.concatenate([rows[:HEAD_DIM].astype(BF16), eye16], axis=0)
        moved = dot(jnp.concatenate([both, both], axis=1), weight)
        return moved[:SLICE] + moved[SLICE:] + rows[HEAD_DIM:]

    state = running[0][0][HEAD_DIM:]
    for g in range(1, groups):
        state = apply(state, running[0][g])
    entries = [state]
    for g in range(groups - 1):
        entries.append(apply(entries[-1], running[1][g]))
    for g in range(groups):
        for t in range(GROUP):
            i = at(g * GROUP + t)
            out = entries[g] if t == 0 else apply(entries[g], comp[peers + g * GROUP + t])
            out_ref[i] = out.astype(BF16)


def entering_states(back, recv):
    peers = recv.shape[0]
    return pl.pallas_call(
        states_kernel,
        in_specs=[
            pl.BlockSpec(memory_space=pltpu.SMEM),
            pl.BlockSpec(memory_space=pltpu.VMEM),
        ],
        out_shape=[
            jax.ShapeDtypeStruct((peers, SLICE, HEAD_DIM), BF16),
            jax.ShapeDtypeStruct((PIECES, HEAD_DIM), F32),
        ],
        scratch_shapes=[pltpu.VMEM((2 * peers, HEAD_DIM + SLICE, HEAD_DIM), F32)],
        compiler_params=limit(16),
        name="entering_states",
    )(back, recv)


def heads_kernel(
    states_hbm, eff_hbm, local_hbm, gain_hbm, out_ref, states_ref, eff_ref, local_ref, gain_ref, sems
):
    pairs = [(states_hbm, states_ref), (gain_hbm, gain_ref)]
    pairs += [(src.at[h], dst.at[h]) for h in (0, 1) for src, dst in ((eff_hbm, eff_ref), (local_hbm, local_ref))]
    copies = fetches(pairs, sems)
    copies[0].wait()
    copies[1].wait()
    for h in (0, 1):
        turned = [
            jnp.concatenate([states_ref[s * 4 + 2 * d + h] for s in range(4)], axis=0) for d in (0, 1)
        ]
        copies[2 + 2 * h].wait()
        copies[3 + 2 * h].wait()
        combined = local_ref[h] + dot_t(eff_ref[h], jnp.concatenate(turned, axis=1))
        scale = lax.rsqrt(jnp.mean(combined * combined, axis=-1, keepdims=True) + EPS)
        out_ref[:, h * HEAD_DIM : (h + 1) * HEAD_DIM] = (combined * scale * gain_ref[...]).astype(BF16)


def head_outputs(states, eff, local, gain):
    rows = eff.shape[1]
    arrays = (states, eff, local, gain)
    return pl.pallas_call(
        heads_kernel,
        in_specs=[HBM] * 4,
        out_specs=VMEM,
        out_shape=jax.ShapeDtypeStruct((rows, 2 * HEAD_DIM), BF16),
        scratch_shapes=[pltpu.VMEM(a.shape, a.dtype) for a in arrays] + [pltpu.SemaphoreType.DMA((6,))],
        compiler_params=limit(60),
        name="head_outputs",
    )(*arrays)


def own_kernel(mine_ref, w_ref, out_ref):
    out_ref[...] = dot(mine_ref[...], w_ref[...])


def update_kernel(sum_ref, other_ref, w_ref, lat_ref, gate_ref, out_ref):
    acc = sum_ref[...] + dot(other_ref[...], w_ref[...])
    for p in range(PIECES):
        cols = slice(p * 128, (p + 1) * 128)
        out_ref[:, cols] = (lat_ref[:, cols].astype(F32) + gate_ref[p : p + 1] * acc[:, cols]).astype(BF16)


def own_half(mine, w):
    return pl.pallas_call(
        own_kernel,
        in_specs=[VMEM] * 2,
        out_specs=VMEM,
        out_shape=jax.ShapeDtypeStruct((mine.shape[0], w.shape[1]), F32),
        compiler_params=limit(16),
        name="own_half",
    )(mine, w)


def update(part, other, w, latent, gate):
    rows = latent.shape[0]
    return pl.pallas_call(
        update_kernel,
        in_specs=[VMEM] * 5,
        out_specs=VMEM,
        out_shape=jax.ShapeDtypeStruct((rows, w.shape[1]), BF16),
        compiler_params=limit(16),
        name="update",
    )(part, other, w, latent, gate)


def body(
    latent,
    context,
    condition,
    context_condition,
    shift_weight,
    scale_weight,
    gate_weight,
    norm_gain,
    query_weight,
    key_weight,
    value_weight,
    write_weight,
    decay_weight,
    write_bias,
    decay_bias,
    log_rate,
    head_gain,
    out_weight,
):
    heads = query_weight.shape[1] // HEAD_DIM
    y, core = lax.axis_index("y"), lax.axis_index("c")
    part = y * 2 + core
    first_head = part * heads
    parts = lax.axis_size(TP)
    peers = lax.axis_size(SP)

    sums, gate_part = partial_sums(
        condition,
        context_condition,
        shift_weight,
        scale_weight,
        gate_weight,
        peers * parts,
    )
    sums = lax.all_to_all(sums, ALL, split_axis=0, concat_axis=0, tiled=True)

    def own(a):
        return lax.dynamic_slice_in_dim(a, first_head, heads, a.ndim - 1)

    gates_w = jnp.concatenate(
        [own(write_weight).reshape(-1, 2 * heads), own(decay_weight).reshape(-1, 2 * heads)], axis=1
    ).T

    ls, cs = row_scales(latent, context)
    gain = norm_gain.reshape(-1, 128)
    head = first_head.astype(jnp.int32).reshape(1)
    mods, k, send, sv, gates = chunk_maps(
        sums,
        gain,
        latent,
        context,
        ls,
        cs,
        key_weight,
        value_weight,
        gates_w,
        head,
        write_bias,
        decay_bias,
        log_rate,
        gate_part,
        parts,
    )
    maps = lax.all_to_all(send, SP, split_axis=0, concat_axis=0, tiled=True)
    eff, local = query_parts(mods, gain, latent, ls, query_weight, k, sv, gates)
    columns = out_weight.shape[1]
    residual = lax.dynamic_slice_in_dim(latent, part * columns, columns, 1)
    block = head_gain.shape[0] * heads

    def ring_rows(which):
        places = [lax.rem(y + off, 4) * 2 + which for off in (0, 3, 1, 2)]
        return jnp.concatenate([lax.dynamic_slice_in_dim(out_weight, p * block, block, 0) for p in places])

    maps, eff, local, residual, w_mine, w_other = lax.optimization_barrier(
        (maps, eff, local, residual, ring_rows(core), ring_rows(1 - core))
    )
    chain = lax.rem(lax.axis_index("x"), 4)
    back = (chain // 2).astype(jnp.int32).reshape(1)
    starts, gate_row = entering_states(back, maps)
    states = lax.all_to_all(starts, SP, split_axis=0, concat_axis=0, tiled=True)
    head_out = head_outputs(states, eff, local, head_gain.reshape(1, -1))

    n = lax.axis_size("y")
    up = [(i, (i + 1) % n) for i in range(n)]
    down = [(i, (i - 1) % n) for i in range(n)]
    cut = head_out.shape[0] // 2
    below = lax.ppermute(head_out, "y", up)
    above = lax.ppermute(head_out, "y", down)
    far_a = lax.ppermute(below[:cut], "y", up)
    far_b = lax.ppermute(above[cut:], "y", down)
    mine = jnp.concatenate([head_out, below, above, jnp.concatenate([far_a, far_b])], axis=1)
    other = lax.ppermute(mine, "c", [(0, 1), (1, 0)])
    half = own_half(mine, w_mine)
    return update(half, other, w_other, residual, gate_row)


def solution(mesh):
    torus = Mesh(mesh.devices.reshape(4, 4, 4, 2), ALL)
    placed = (
        P(SP, None),
        P(SP, None),
        P(SP),
        P(SP),
        P(SP, TP),
        P(SP, TP),
        P(SP, TP),
        P(),
        P(None, TP),
        P(None, TP),
        P(None, TP),
        P(),
        P(),
        P(),
        P(),
        P(),
        P(),
        P(None, TP),
    )
    return jax.shard_map(body, mesh=torus, in_specs=placed, out_specs=P(SP, TP), check_vma=False)
```

```python
import functools

import jax
import jax.numpy as jnp
from jax import lax
from jax.experimental import pallas as pl
from jax.experimental.pallas import tpu as pltpu
from jax.sharding import Mesh
from jax.sharding import PartitionSpec as P

HEAD_DIM = 128
BLOCK = 128
SP = ("z", "x")
TP = ("y", "c")
ALL = ("z", "x", "y", "c")
SLICE = 32
EPS = 0.0001
F32 = jnp.float32
BF16 = jnp.bfloat16


def dot(a, b):
    return jnp.dot(a, b, preferred_element_type=F32)


def dot_t(a, b):
    return lax.dot_general(a, b, (((1,), (1,)), ((), ())), preferred_element_type=F32)


def t_dot(a, b):
    return lax.dot_general(a, b, (((0,), (0,)), ((), ())), preferred_element_type=F32)


def running_sums(mask, x):
    hi = x.astype(BF16)
    rest = x - hi.astype(F32)
    mid = rest.astype(BF16)
    low = (rest - mid.astype(F32)).astype(BF16)
    n = x.shape[1]
    out = dot(mask, jnp.concatenate([hi, mid, low], axis=1))
    return out[:, :n] + out[:, n : 2 * n] + out[:, 2 * n :]


def iotas(n):
    shape = (n, n)
    return lax.broadcasted_iota(jnp.int32, shape, 0), lax.broadcasted_iota(jnp.int32, shape, 1)


def unit(x):
    x = x.astype(F32)
    return x * lax.rsqrt(jnp.sum(x * x, axis=-1, keepdims=True) + EPS)


def log1p_small(e):
    series = e * (1.0 - e * (0.5 - e * (1.0 / 3.0 - 0.25 * e)))
    return jnp.where(e < 0.01, series, jnp.log(1.0 + e))


def softplus(x):
    return jnp.maximum(x, 0.0) + log1p_small(jnp.exp(-jnp.abs(x)))


VMEM = pl.BlockSpec(memory_space=pltpu.VMEM)
PIECES = 4


def limit(mib):
    return pltpu.CompilerParams(vmem_limit_bytes=mib * 1024 * 1024)


HBM = pl.BlockSpec(memory_space=pltpu.HBM)


def fetches(pairs, sems):
    copies = [pltpu.make_async_copy(src, dst, sems.at[i]) for i, (src, dst) in enumerate(pairs)]
    for c in copies:
        c.start()
    return copies


def partial_sums_kernel(
    cond_hbm, ctx_cond_hbm, shift_ref, scale_ref, gate_ref, out_ref, gate_out,
    cond_ref, ctx_cond_ref, w_shift, w_scale, w_gate, sems,
):
    pairs = ((cond_hbm, cond_ref), (ctx_cond_hbm, ctx_cond_ref))
    copies = fetches(pairs + ((shift_ref, w_shift), (scale_ref, w_scale), (gate_ref, w_gate)), sems)
    copies[0].wait()
    copies[1].wait()
    copies = copies[2:]
    n = cond_ref.shape[0]
    u = jnp.concatenate([r[...].astype(F32).reshape(1, n) for r in (cond_ref, ctx_cond_ref)] * 4, axis=0)
    s = (u * jax.nn.sigmoid(u)).astype(BF16)
    every = []
    for copy, w in zip(copies[:2], (w_shift, w_scale)):
        copy.wait()
        sums = dot(s, w[...])
        every += [sums[0:1], sums[1:2]]
    pieces = [r[:, p * 128 : (p + 1) * 128] for r in every for p in range(PIECES)]
    block = jnp.concatenate(pieces, axis=0).astype(BF16)
    for j in range(out_ref.shape[0]):
        out_ref[j] = block
    copies[2].wait()
    gate = dot(s, w_gate[...])[0:1]
    gate = jnp.concatenate([gate[:, p * 128 : (p + 1) * 128] for p in range(PIECES)], axis=0)
    hi = gate.astype(BF16)
    gate_out[...] = jnp.concatenate([hi, (gate - hi.astype(F32)).astype(BF16)], axis=0)


def partial_sums(cond, ctx_cond, shift, scale, gate, peers):
    return pl.pallas_call(
        partial_sums_kernel,
        in_specs=[HBM] * 5,
        out_specs=[VMEM] * 2,
        out_shape=[
            jax.ShapeDtypeStruct((peers, 4 * PIECES, 128), BF16),
            jax.ShapeDtypeStruct((2 * PIECES, 128), BF16),
        ],
        scratch_shapes=[pltpu.VMEM(cond.shape, BF16)] * 2
        + [pltpu.VMEM(shift.shape, BF16)] * 3
        + [pltpu.SemaphoreType.DMA((5,))],
        compiler_params=limit(60),
        name="partial_sums",
    )(cond, ctx_cond, shift, scale, gate)


def row_scale_kernel(lat_ref, ctx_ref, lat_out, ctx_out):
    def scale(ref):
        x = ref[...].astype(F32)
        s = lax.rsqrt(jnp.mean(x * x, axis=-1, keepdims=True) + EPS)
        return jnp.broadcast_to(s, (x.shape[0], 128))

    lat_out[...] = scale(lat_ref)

    @pl.when(pl.program_id(0) == 0)
    def _():
        ctx_out[...] = scale(ctx_ref)


def row_scales(latent, context):
    rows, width = latent.shape
    crows = context.shape[0]
    step = 128
    return pl.pallas_call(
        row_scale_kernel,
        grid=(rows // step,),
        in_specs=[
            pl.BlockSpec((step, width), lambda i: (i, 0)),
            pl.BlockSpec((crows, width), lambda i: (0, 0)),
        ],
        out_specs=[
            pl.BlockSpec((step, 128), lambda i: (i, 0)),
            pl.BlockSpec((crows, 128), lambda i: (0, 0)),
        ],
        out_shape=[
            jax.ShapeDtypeStruct((rows, 128), F32),
            jax.ShapeDtypeStruct((crows, 128), F32),
        ],
        compiler_params=limit(8),
        name="row_scales",
    )(latent, context)


def modulate(i, mods_ref, gain_ref, pieces, m_ref):
    for p in range(PIECES):
        f = i * PIECES + p
        cols = pl.ds(pl.multiple_of(f * 128, 128), 128)
        gain = gain_ref[pl.ds(f, 1)]
        for ref, scale, r, at in pieces:
            n = ref.shape[0]
            shift = mods_ref[i, r * PIECES + p : r * PIECES + p + 1]
            grow = gain * (1.0 + mods_ref[i, (2 + r) * PIECES + p : (2 + r) * PIECES + p + 1])
            x = ref[:, cols].astype(F32)
            m_ref[at : at + n, cols] = (x * scale[...] * grow + shift).astype(BF16)


def project(recv_ref, gain_ref, ls_ref, cs_ref, queue, small, mods_ref, lat_ref, ctx_ref, m_ref, k_ref, v_ref, g_ref, weights):
    parts = mods_ref.shape[0]
    rows = lat_ref.shape[0]
    peers = recv_ref.shape[0] // parts
    for c in queue:
        c.start()
    for c in queue[:small]:
        c.wait()
    for t in range(parts):
        total = recv_ref[t].astype(F32)
        for j in range(1, peers):
            total = total + recv_ref[j * parts + t].astype(F32)
        mods_ref[t] = total
    for i in range(parts):
        queue[small + i].wait()
        modulate(i, mods_ref, gain_ref, ((lat_ref, ls_ref, 0, 0), (ctx_ref, cs_ref, 1, rows)), m_ref)
    wk, wv, wg = weights
    queue[small + parts].wait()
    k_ref[...] = dot(m_ref[...], wk[...]).astype(BF16)
    queue[small + parts + 1].wait()
    v_ref[...] = dot(m_ref[...], wv[...]).astype(BF16)
    g_ref[...] = dot_t(m_ref[...], wg[...]).astype(BF16)


def maps_kernel(
    recv_hbm, gain_hbm, lat_hbm, ctx_hbm, ls_hbm, cs_hbm, wk_hbm, wv_hbm, wg_hbm, head_ref, wb_ref, db_ref, lr_ref, part_hbm,
    mods_hbm, k_hbm, send_hbm, sv_hbm, gates_hbm,
    recv_ref, gain_ref, lat_ref, ctx_ref, ls_ref, cs_ref, wk, wv, wg, part_ref,
    mods_ref, k_ref, send_ref, sv_ref, gates_ref, m_ref, v_ref, g_ref, low, inv, uw, kn, in_sems, sems, sv_sems,
):
    parts = mods_ref.shape[0]
    step = lat_ref.shape[1] // parts
    cuts = [slice(i * step, (i + 1) * step) for i in range(parts)]
    loads = [(recv_hbm, recv_ref), (gain_hbm, gain_ref), (ls_hbm, ls_ref), (cs_hbm, cs_ref), (ctx_hbm, ctx_ref)]
    loads += [(part_hbm, part_ref), (wg_hbm, wg)]
    small = len(loads)
    loads += [(lat_hbm.at[:, c], lat_ref.at[:, c]) for c in cuts]
    loads += [(wk_hbm, wk), (wv_hbm, wv)]
    queue = [pltpu.make_async_copy(src, dst, in_sems.at[i]) for i, (src, dst) in enumerate(loads)]
    project(
        recv_ref, gain_ref, ls_ref, cs_ref, queue, small, mods_ref, lat_ref, ctx_ref, m_ref, k_ref, v_ref, g_ref, (wk, wv, wg)
    )

    nblk = (k_ref.shape[0] - 64) // BLOCK
    lats = nblk * BLOCK
    lane = lax.broadcasted_iota(jnp.int32, (1, 8), 1)
    bias = jnp.zeros((1, 8), F32)
    speed = jnp.zeros((1, 8), F32)
    for c in range(4):
        d, h = c // 2, head_ref[0] + c % 2
        bias = jnp.where(lane == c, wb_ref[d, h], jnp.where(lane == 4 + c, db_ref[d, h], bias))
        speed = jnp.where(lane == 4 + c, lr_ref[d, h], speed)
    for j in range(send_ref.shape[0]):
        send_ref[j, 2 * BLOCK + 2 * SLICE :] = part_ref[...]
    ri, ci = iotas(BLOCK)
    apart = ri ^ ci
    eye = (ri == ci).astype(F32)
    pre = g_ref[...].astype(F32) + bias
    rates = jax.nn.sigmoid(pre)
    logs = -jnp.exp(speed) * softplus(pre)
    gap = jnp.zeros((pre.shape[0], 120), F32)
    rates = jnp.concatenate([rates, gap], axis=1)
    logs = jnp.concatenate([logs, gap], axis=1)
    below = ri >= ci
    for h in (0, 1):
        kn[h] = unit(k_ref[:, h * HEAD_DIM : (h + 1) * HEAD_DIM])
    strict = (ri > ci, ri < ci)

    def system(slot, gram, d, rate, col, rowv):
        spread = jnp.where(strict[d], col - rowv, 0.0)
        s = jnp.where(strict[d], gram * (-rate) * jnp.exp(spread), 0.0)
        low[slot] = s.astype(BF16)
        inv[slot] = (eye + jnp.where(apart == 1, s, 0.0)).astype(BF16)

    half = BLOCK // 2
    same = apart < half
    crate = jnp.concatenate([rates[lats:]] * 2, axis=0)
    clog = jnp.concatenate([logs[lats:]] * 2, axis=0)
    cfwd = running_sums((below & same).astype(BF16), clog)
    top = lax.broadcasted_iota(jnp.int32, (BLOCK, 1), 0) < half
    cbwd = clog - cfwd + jnp.where(top, cfwd[half - 1 : half], cfwd[BLOCK - 1 :])
    cr = [jnp.where(top, crate[:, 2 * d : 2 * d + 1], crate[:, 2 * d + 1 : 2 * d + 2]) for d in (0, 1)]
    cg = [
        jnp.where(top, c[:, 4 + 2 * d : 5 + 2 * d], c[:, 5 + 2 * d : 6 + 2 * d])
        for d, c in ((0, cfwd), (1, cbwd))
    ]
    cgt = jnp.where(ci == 0, cg[0], cg[1]).T
    ck = [kn[h, lats:] for h in (0, 1)]
    ckk = jnp.concatenate(ck, axis=0)
    cvv = jnp.concatenate(
        [v_ref[lats:, h * HEAD_DIM : (h + 1) * HEAD_DIM].astype(F32) for h in (0, 1)], axis=0
    )
    ckb = ckk.astype(BF16)
    cgram = jnp.where(same, dot_t(ckb, ckb), 0.0)
    for d in (0, 1):
        system(4 * nblk + d, cgram, d, cr[d], cg[d], cgt[d : d + 1])

    keys = [[None] * nblk for _ in (0, 1)]
    for b in range(nblk):
        rows = slice(b * BLOCK, (b + 1) * BLOCK)
        fwd = running_sums(below.astype(BF16), logs[rows])
        bwd = logs[rows] - fwd + fwd[BLOCK - 1 :]
        both = jnp.where(ci < 4, rates[rows], jnp.where(ci < 6, fwd, bwd))
        turned = both.T
        gates_ref[b, 0] = both
        gates_ref[b, 1] = turned
        for h in (0, 1):
            kb = kn[h, rows].astype(BF16)
            gram = dot_t(kb, kb)
            for d in (0, 1):
                c = 2 * d + h
                system(c * nblk + b, gram, d, both[:, c : c + 1], both[:, 4 + c : 5 + c], turned[4 + c : 5 + c])

    count = 4 * nblk + 2

    def level(i, size):
        pick = (apart >= size) & (apart < 2 * size)
        halves = []
        for s in range(count):
            t = inv[s]
            m = jnp.where(pick, low[s], jnp.zeros((), BF16))
            halves.append(dot(t, m).astype(BF16))
        for s in range(count):
            t = inv[s]
            inv[s] = t + dot(halves[s], t).astype(BF16)
        return size * 2

    lax.fori_loop(0, 6, level, jnp.int32(2))

    for d in (0, 1):
        side = jnp.concatenate([cvv * cr[d], ckk * (cr[d] * jnp.exp(cg[d]))], axis=1)
        solved = dot(inv[4 * nblk + d], side.astype(BF16))
        packed = jnp.concatenate([-solved[:, HEAD_DIM:], solved[:, :HEAD_DIM]], axis=1).astype(BF16)
        for h in (0, 1):
            c = 2 * d + h
            rows = slice(h * half, (h + 1) * half)
            end = (h * half + half - 1) if d == 0 else h * half
            last = cg[d][end : end + 1]
            late = ckk[rows] * jnp.exp(last - cg[d][rows])
            ab = t_dot(late.astype(BF16), packed[rows])
            change = (ab[:, :HEAD_DIM] + eye * (jnp.exp(last) - 1.0)).astype(BF16)
            add = ab[:, HEAD_DIM:].T.astype(BF16)
            for s in range(4):
                send_ref[s * 4 + c, BLOCK : 2 * BLOCK] = change
                send_ref[s * 4 + c, 2 * BLOCK + SLICE : 2 * BLOCK + 2 * SLICE] = add[s * SLICE : (s + 1) * SLICE]

    lat_rows = (slice(0, BLOCK), slice(2 * BLOCK, 2 * BLOCK + SLICE))
    ctx_rows = (slice(BLOCK, 2 * BLOCK), slice(2 * BLOCK + SLICE, send_ref.shape[1]))
    pairs = [(gates_ref, gates_hbm), (k_ref, k_hbm), (mods_ref, mods_hbm)] + [(send_ref.at[:, r], send_hbm.at[:, r]) for r in ctx_rows]
    waiting = fetches(pairs, sems)

    for b in range(nblk):
        rows = slice(b * BLOCK, (b + 1) * BLOCK)
        both = gates_ref[b, 0]
        for h in (0, 1):
            cols = slice(h * HEAD_DIM, (h + 1) * HEAD_DIM)
            kk = kn[h, rows]
            vv = v_ref[rows, cols].astype(F32)
            for d in (0, 1):
                c = 2 * d + h
                rate = both[:, c : c + 1]
                g = both[:, 4 + c : 5 + c]
                side = jnp.concatenate([kk * (rate * jnp.exp(g)), vv * rate], axis=1).astype(BF16)
                uw[c * nblk + b] = dot(inv[c * nblk + b], side)

    start = jnp.concatenate([eye, jnp.zeros_like(eye)], axis=1)
    states = [start] * 4
    for t in range(nblk):
        for c in range(4):
            d, h = c // 2, c % 2
            b = t if d == 0 else nblk - 1 - t
            rows = slice(b * BLOCK, (b + 1) * BLOCK)
            state = states[c]
            sb = state.astype(BF16)
            sv_ref[c * nblk + b, :BLOCK] = sb
            solved = uw[c * nblk + b]
            moved = dot(solved[:, :HEAD_DIM].astype(BF16), sb)
            fresh = jnp.concatenate(
                [-moved[:, :HEAD_DIM], solved[:, HEAD_DIM:] - moved[:, HEAD_DIM:]], axis=1
            ).astype(BF16)
            sv_ref[c * nblk + b, BLOCK:] = fresh
            g = gates_ref[b, 0][:, 4 + c : 5 + c]
            end = BLOCK - 1 if d == 0 else 0
            last = g[end : end + 1]
            late = (kn[h, rows] * jnp.exp(last - g)).astype(BF16)
            states[c] = state * jnp.exp(last) + t_dot(late, fresh)
        for c in range(4):
            b = c * nblk + (t if c < 2 else nblk - 1 - t)
            copy = pltpu.make_async_copy(sv_ref.at[b], sv_hbm.at[b], sv_sems.at[b])
            copy.start()
            waiting.append(copy)
    for c in range(4):
        change = (states[c][:, :HEAD_DIM] - eye).astype(BF16)
        add = states[c][:, HEAD_DIM:].T.astype(BF16)
        for s in range(4):
            send_ref[s * 4 + c, :BLOCK] = change
            send_ref[s * 4 + c, 2 * BLOCK : 2 * BLOCK + SLICE] = add[s * SLICE : (s + 1) * SLICE]
    late_pairs = [(send_ref.at[:, r], send_hbm.at[:, r]) for r in lat_rows]
    for i, (src, dst) in enumerate(late_pairs):
        copy = pltpu.make_async_copy(src, dst, sems.at[len(pairs) + i])
        copy.start()
        waiting.append(copy)
    for copy in waiting:
        copy.wait()


def chunk_maps(recv, gain, latent, context, ls, cs, wk, wv, wg, head, wb, db, lr, part, parts):
    rows, width = latent.shape
    every = rows + context.shape[0]
    ncol = wk.shape[1]
    nblk = rows // BLOCK
    count = 4 * nblk
    outs = [
        jax.ShapeDtypeStruct((16, 2 * BLOCK + 2 * SLICE + 2 * PIECES, HEAD_DIM), BF16),
        jax.ShapeDtypeStruct((count, 2 * BLOCK, 2 * HEAD_DIM), BF16),
        jax.ShapeDtypeStruct((nblk, 2, BLOCK, 128), F32),
    ]
    outs = [
        jax.ShapeDtypeStruct((parts, 4 * PIECES, 128), F32),
        jax.ShapeDtypeStruct((every, ncol), BF16),
    ] + outs
    smem = pl.BlockSpec(memory_space=pltpu.SMEM)
    loaded = (recv, gain, latent, context, ls, cs, wk, wv, wg, part)
    return pl.pallas_call(
        maps_kernel,
        in_specs=[HBM] * 9 + [smem] * 4 + [HBM],
        out_specs=[HBM] * 5,
        out_shape=outs,
        scratch_shapes=[pltpu.VMEM(a.shape, a.dtype) for a in loaded]
        + [pltpu.VMEM(o.shape, o.dtype) for o in outs]
        + [
            pltpu.VMEM((every, width), BF16),
            pltpu.VMEM((every, ncol), BF16),
            pltpu.VMEM((every, wg.shape[0]), BF16),
            pltpu.VMEM((count + 2, BLOCK, BLOCK), BF16),
            pltpu.VMEM((count + 2, BLOCK, BLOCK), BF16),
            pltpu.VMEM((count, BLOCK, 2 * HEAD_DIM), F32),
            pltpu.VMEM((2, every, HEAD_DIM), F32),
            pltpu.SemaphoreType.DMA((parts + 9,)),
            pltpu.SemaphoreType.DMA((7,)),
            pltpu.SemaphoreType.DMA((count,)),
        ],
        compiler_params=limit(60),
        name="chunk_maps",
    )(recv, gain, latent, context, ls, cs, wk, wv, wg, head, wb, db, lr, part)


def query_kernel(
    mods_ref, gain_ref, lat_ref, ls_ref, wq_ref, k_ref, sv_ref, gates_ref, eff_ref, local_ref, m_ref, q_ref
):
    nblk = q_ref.shape[0] // BLOCK

    def fill(i, carry):
        modulate(i, mods_ref, gain_ref, ((lat_ref, ls_ref, 0, 0),), m_ref)
        return carry

    lax.fori_loop(0, mods_ref.shape[0], fill, 0)
    q_ref[...] = dot(m_ref[...], wq_ref[...]).astype(BF16)
    ri, ci = iotas(BLOCK)
    seen = (ri >= ci, ri <= ci)
    for b in range(nblk):
        rows = slice(b * BLOCK, (b + 1) * BLOCK)
        both = gates_ref[b, 0]
        turned = gates_ref[b, 1]
        for h in (0, 1):
            cols = slice(h * HEAD_DIM, (h + 1) * HEAD_DIM)
            qq = unit(q_ref[rows, cols]) * HEAD_DIM**-0.5
            kb = unit(k_ref[rows, cols]).astype(BF16)
            scores = dot_t(qq.astype(BF16), kb)
            local = None
            for d in (0, 1):
                c = 2 * d + h
                g = both[:, 4 + c : 5 + c]
                spread = jnp.where(seen[d], g - turned[4 + c : 5 + c], 0.0)
                decayed = jnp.where(seen[d], scores * jnp.exp(spread), 0.0)
                side = jnp.concatenate([qq * jnp.exp(g), decayed], axis=1).astype(BF16)
                out = dot(side, sv_ref[c * nblk + b])
                eff_ref[h, rows, d * HEAD_DIM : (d + 1) * HEAD_DIM] = out[:, :HEAD_DIM].astype(BF16)
                local = out[:, HEAD_DIM:] if local is None else local + out[:, HEAD_DIM:]
            local_ref[h, rows] = local


def query_parts(mods, gain, latent, ls, wq, k, sv, gates):
    rows = latent.shape[0]
    return pl.pallas_call(
        query_kernel,
        in_specs=[VMEM] * 8,
        out_specs=[VMEM] * 2,
        out_shape=[
            jax.ShapeDtypeStruct((2, rows, 2 * HEAD_DIM), BF16),
            jax.ShapeDtypeStruct((2, rows, HEAD_DIM), F32),
        ],
        scratch_shapes=[pltpu.VMEM(latent.shape, BF16), pltpu.VMEM((rows, wq.shape[1]), BF16)],
        compiler_params=limit(60),
        name="query_parts",
    )(mods, gain, latent, ls, wq, k, sv, gates)


GROUP = 4


def states_kernel(back_ref, recv_ref, out_ref, gate_ref, comp):
    back = back_ref[0]
    peers = recv_ref.shape[0]
    gate = recv_ref[0, 2 * BLOCK + 2 * SLICE :].astype(F32)
    for j in range(1, peers):
        gate = gate + recv_ref[j, 2 * BLOCK + 2 * SLICE :].astype(F32)
    gate_ref[...] = gate[:PIECES] + gate[PIECES:]
    groups = peers // GROUP
    ri, ci = iotas(HEAD_DIM)
    eye = (ri == ci).astype(F32)

    def at(t):
        return jnp.where(back == 1, peers - 1 - t, t)

    def through(rows, weight):
        hi = rows.astype(BF16)
        lo = (rows - hi.astype(F32)).astype(BF16)
        n = rows.shape[0]
        moved = dot_t(jnp.concatenate([hi, lo], axis=0), weight)
        return moved[:n] + moved[n:]

    still = jnp.concatenate([eye, jnp.zeros((SLICE, HEAD_DIM), F32)], axis=0)
    running = [[jnp.zeros_like(still)] * groups for _ in (0, 1)]
    for t in range(GROUP):
        for kind in (0, 1):
            base = BLOCK * (1 - kind)
            extra = 2 * BLOCK + SLICE * (1 - kind)
            for g in range(groups):
                i = at(g * GROUP + t)
                rows = running[kind][g]
                moved = through(rows + still, recv_ref[i, base : base + BLOCK])
                add = recv_ref[i, extra : extra + SLICE].astype(F32)
                rows = rows + moved
                rows = jnp.concatenate([rows[:HEAD_DIM], rows[HEAD_DIM:] + add], axis=0)
                running[kind][g] = rows
                if t < GROUP - 1:
                    comp[kind * peers + g * GROUP + t + 1] = rows

    eye16 = eye.astype(BF16)

    def apply(state, rows):
        hi = state.astype(BF16)
        lo = (state - hi.astype(F32)).astype(BF16)
        both = jnp.concatenate([hi, lo], axis=0)
        weight = jnp.concatenate([rows[:HEAD_DIM].astype(BF16), eye16], axis=0)
        moved = dot(jnp.concatenate([both, both], axis=1), weight)
        return moved[:SLICE] + moved[SLICE:] + rows[HEAD_DIM:]

    state = running[0][0][HEAD_DIM:]
    for g in range(1, groups):
        state = apply(state, running[0][g])
    entries = [state]
    for g in range(groups - 1):
        entries.append(apply(entries[-1], running[1][g]))
    for g in range(groups):
        for t in range(GROUP):
            i = at(g * GROUP + t)
            out = entries[g] if t == 0 else apply(entries[g], comp[peers + g * GROUP + t])
            out_ref[i] = out.astype(BF16)


def entering_states(back, recv):
    peers = recv.shape[0]
    return pl.pallas_call(
        states_kernel,
        in_specs=[
            pl.BlockSpec(memory_space=pltpu.SMEM),
            pl.BlockSpec(memory_space=pltpu.VMEM),
        ],
        out_shape=[
            jax.ShapeDtypeStruct((peers, SLICE, HEAD_DIM), BF16),
            jax.ShapeDtypeStruct((PIECES, HEAD_DIM), F32),
        ],
        scratch_shapes=[pltpu.VMEM((2 * peers, HEAD_DIM + SLICE, HEAD_DIM), F32)],
        compiler_params=limit(16),
        name="entering_states",
    )(back, recv)


def heads_kernel(
    states_hbm, eff_hbm, local_hbm, gain_hbm, out_ref, states_ref, eff_ref, local_ref, gain_ref, sems
):
    pairs = [(states_hbm, states_ref), (gain_hbm, gain_ref)]
    pairs += [(src.at[h], dst.at[h]) for h in (0, 1) for src, dst in ((eff_hbm, eff_ref), (local_hbm, local_ref))]
    copies = fetches(pairs, sems)
    copies[0].wait()
    copies[1].wait()
    for h in (0, 1):
        turned = [
            jnp.concatenate([states_ref[s * 4 + 2 * d + h] for s in range(4)], axis=0) for d in (0, 1)
        ]
        copies[2 + 2 * h].wait()
        copies[3 + 2 * h].wait()
        combined = local_ref[h] + dot_t(eff_ref[h], jnp.concatenate(turned, axis=1))
        scale = lax.rsqrt(jnp.mean(combined * combined, axis=-1, keepdims=True) + EPS)
        out_ref[:, h * HEAD_DIM : (h + 1) * HEAD_DIM] = (combined * scale * gain_ref[...]).astype(BF16)


def head_outputs(states, eff, local, gain):
    rows = eff.shape[1]
    arrays = (states, eff, local, gain)
    return pl.pallas_call(
        heads_kernel,
        in_specs=[HBM] * 4,
        out_specs=VMEM,
        out_shape=jax.ShapeDtypeStruct((rows, 2 * HEAD_DIM), BF16),
        scratch_shapes=[pltpu.VMEM(a.shape, a.dtype) for a in arrays] + [pltpu.SemaphoreType.DMA((6,))],
        compiler_params=limit(60),
        name="head_outputs",
    )(*arrays)


def own_kernel(mine_ref, w_ref, out_ref):
    out_ref[...] = dot(mine_ref[...], w_ref[...])


def update_kernel(sum_ref, other_ref, w_ref, lat_ref, gate_ref, out_ref):
    acc = sum_ref[...] + dot(other_ref[...], w_ref[...])
    for p in range(PIECES):
        cols = slice(p * 128, (p + 1) * 128)
        out_ref[:, cols] = (lat_ref[:, cols].astype(F32) + gate_ref[p : p + 1] * acc[:, cols]).astype(BF16)


def own_half(mine, w):
    return pl.pallas_call(
        own_kernel,
        in_specs=[VMEM] * 2,
        out_specs=VMEM,
        out_shape=jax.ShapeDtypeStruct((mine.shape[0], w.shape[1]), F32),
        compiler_params=limit(16),
        name="own_half",
    )(mine, w)


def update(part, other, w, latent, gate):
    rows = latent.shape[0]
    return pl.pallas_call(
        update_kernel,
        in_specs=[VMEM] * 5,
        out_specs=VMEM,
        out_shape=jax.ShapeDtypeStruct((rows, w.shape[1]), BF16),
        compiler_params=limit(16),
        name="update",
    )(part, other, w, latent, gate)


def body(
    latent,
    context,
    condition,
    context_condition,
    shift_weight,
    scale_weight,
    gate_weight,
    norm_gain,
    query_weight,
    key_weight,
    value_weight,
    write_weight,
    decay_weight,
    write_bias,
    decay_bias,
    log_rate,
    head_gain,
    out_weight,
):
    heads = query_weight.shape[1] // HEAD_DIM
    y, core = lax.axis_index("y"), lax.axis_index("c")
    part = y * 2 + core
    first_head = part * heads
    parts = lax.axis_size(TP)
    peers = lax.axis_size(SP)

    sums, gate_part = partial_sums(
        condition,
        context_condition,
        shift_weight,
        scale_weight,
        gate_weight,
        peers * parts,
    )
    sums = lax.all_to_all(sums, ALL, split_axis=0, concat_axis=0, tiled=True)

    def own(a):
        return lax.dynamic_slice_in_dim(a, first_head, heads, a.ndim - 1)

    gates_w = jnp.concatenate(
        [own(write_weight).reshape(-1, 2 * heads), own(decay_weight).reshape(-1, 2 * heads)], axis=1
    ).T

    ls, cs = row_scales(latent, context)
    gain = norm_gain.reshape(-1, 128)
    head = first_head.astype(jnp.int32).reshape(1)
    mods, k, send, sv, gates = chunk_maps(
        sums,
        gain,
        latent,
        context,
        ls,
        cs,
        key_weight,
        value_weight,
        gates_w,
        head,
        write_bias,
        decay_bias,
        log_rate,
        gate_part,
        parts,
    )
    maps = lax.all_to_all(send, SP, split_axis=0, concat_axis=0, tiled=True)
    eff, local = query_parts(mods, gain, latent, ls, query_weight, k, sv, gates)
    columns = out_weight.shape[1]
    residual = lax.dynamic_slice_in_dim(latent, part * columns, columns, 1)
    block = head_gain.shape[0] * heads

    def ring_rows(which):
        places = [lax.rem(y + off, 4) * 2 + which for off in (0, 3, 1, 2)]
        return jnp.concatenate([lax.dynamic_slice_in_dim(out_weight, p * block, block, 0) for p in places])

    maps, eff, local, residual, w_mine, w_other = lax.optimization_barrier(
        (maps, eff, local, residual, ring_rows(core), ring_rows(1 - core))
    )
    chain = lax.rem(lax.axis_index("x"), 4)
    back = (chain // 2).astype(jnp.int32).reshape(1)
    starts, gate_row = entering_states(back, maps)
    states = lax.all_to_all(starts, SP, split_axis=0, concat_axis=0, tiled=True)
    head_out = head_outputs(states, eff, local, head_gain.reshape(1, -1))

    n = lax.axis_size("y")
    up = [(i, (i + 1) % n) for i in range(n)]
    down = [(i, (i - 1) % n) for i in range(n)]
    cut = head_out.shape[0] // 2
    top, low = head_out[:cut], head_out[cut:]
    below_top = lax.ppermute(top, "y", up)
    above_low = lax.ppermute(low, "y", down)
    below_low = lax.ppermute(low, "y", up)
    above_top = lax.ppermute(top, "y", down)
    far_top = lax.ppermute(below_top, "y", up)
    far_low = lax.ppermute(above_low, "y", down)
    pieces = ((below_top, below_low), (above_top, above_low), (far_top, far_low))
    mine = jnp.concatenate([head_out] + [jnp.concatenate(p) for p in pieces], axis=1)
    other = lax.ppermute(mine, "c", [(0, 1), (1, 0)])
    half = own_half(mine, w_mine)
    return update(half, other, w_other, residual, gate_row)


def solution(mesh):
    torus = Mesh(mesh.devices.reshape(4, 4, 4, 2), ALL)
    placed = (
        P(SP, None),
        P(SP, None),
        P(SP),
        P(SP),
        P(SP, TP),
        P(SP, TP),
        P(SP, TP),
        P(),
        P(None, TP),
        P(None, TP),
        P(None, TP),
        P(),
        P(),
        P(),
        P(),
        P(),
        P(),
        P(None, TP),
    )
    return jax.shard_map(body, mesh=torus, in_specs=placed, out_specs=P(SP, TP), check_vma=False)
```

```python
import functools

import jax
import jax.numpy as jnp
from jax import lax
from jax.experimental import pallas as pl
from jax.experimental.pallas import tpu as pltpu
from jax.sharding import Mesh
from jax.sharding import PartitionSpec as P

HEAD_DIM = 128
BLOCK = 128
SP = ("z", "x")
TP = ("y", "c")
ALL = ("z", "x", "y", "c")
SLICE = 32
EPS = 0.0001
F32 = jnp.float32
BF16 = jnp.bfloat16


def dot(a, b):
    return jnp.dot(a, b, preferred_element_type=F32)


def dot_t(a, b):
    return lax.dot_general(a, b, (((1,), (1,)), ((), ())), preferred_element_type=F32)


def t_dot(a, b):
    return lax.dot_general(a, b, (((0,), (0,)), ((), ())), preferred_element_type=F32)


def running_sums(mask, x):
    hi = x.astype(BF16)
    rest = x - hi.astype(F32)
    mid = rest.astype(BF16)
    low = (rest - mid.astype(F32)).astype(BF16)
    n = x.shape[1]
    out = dot(mask, jnp.concatenate([hi, mid, low], axis=1))
    return out[:, :n] + out[:, n : 2 * n] + out[:, 2 * n :]


def iotas(n):
    shape = (n, n)
    return lax.broadcasted_iota(jnp.int32, shape, 0), lax.broadcasted_iota(jnp.int32, shape, 1)


def unit(x):
    x = x.astype(F32)
    return x * lax.rsqrt(jnp.sum(x * x, axis=-1, keepdims=True) + EPS)


def log1p_small(e):
    series = e * (1.0 - e * (0.5 - e * (1.0 / 3.0 - 0.25 * e)))
    return jnp.where(e < 0.01, series, jnp.log(1.0 + e))


def softplus(x):
    return jnp.maximum(x, 0.0) + log1p_small(jnp.exp(-jnp.abs(x)))


VMEM = pl.BlockSpec(memory_space=pltpu.VMEM)
PIECES = 4


def limit(mib):
    return pltpu.CompilerParams(vmem_limit_bytes=mib * 1024 * 1024)


HBM = pl.BlockSpec(memory_space=pltpu.HBM)


def fetches(pairs, sems):
    copies = [pltpu.make_async_copy(src, dst, sems.at[i]) for i, (src, dst) in enumerate(pairs)]
    for c in copies:
        c.start()
    return copies


def partial_sums_kernel(
    cond_hbm, ctx_cond_hbm, shift_ref, scale_ref, gate_ref, out_ref, gate_out,
    cond_ref, ctx_cond_ref, w_shift, w_scale, w_gate, sems,
):
    pairs = ((cond_hbm, cond_ref), (ctx_cond_hbm, ctx_cond_ref))
    copies = fetches(pairs + ((shift_ref, w_shift), (scale_ref, w_scale), (gate_ref, w_gate)), sems)
    copies[0].wait()
    copies[1].wait()
    copies = copies[2:]
    n = cond_ref.shape[0]
    u = jnp.concatenate([r[...].astype(F32).reshape(1, n) for r in (cond_ref, ctx_cond_ref)] * 4, axis=0)
    s = (u * jax.nn.sigmoid(u)).astype(BF16)
    every = []
    for copy, w in zip(copies[:2], (w_shift, w_scale)):
        copy.wait()
        sums = dot(s, w[...])
        every += [sums[0:1], sums[1:2]]
    pieces = [r[:, p * 128 : (p + 1) * 128] for r in every for p in range(PIECES)]
    block = jnp.concatenate(pieces, axis=0).astype(BF16)
    for j in range(out_ref.shape[0]):
        out_ref[j] = block
    copies[2].wait()
    gate = dot(s, w_gate[...])[0:1]
    gate = jnp.concatenate([gate[:, p * 128 : (p + 1) * 128] for p in range(PIECES)], axis=0)
    hi = gate.astype(BF16)
    gate_out[...] = jnp.concatenate([hi, (gate - hi.astype(F32)).astype(BF16)], axis=0)


def partial_sums(cond, ctx_cond, shift, scale, gate, peers):
    return pl.pallas_call(
        partial_sums_kernel,
        in_specs=[HBM] * 5,
        out_specs=[VMEM] * 2,
        out_shape=[
            jax.ShapeDtypeStruct((peers, 4 * PIECES, 128), BF16),
            jax.ShapeDtypeStruct((2 * PIECES, 128), BF16),
        ],
        scratch_shapes=[pltpu.VMEM(cond.shape, BF16)] * 2
        + [pltpu.VMEM(shift.shape, BF16)] * 3
        + [pltpu.SemaphoreType.DMA((5,))],
        compiler_params=limit(60),
        name="partial_sums",
    )(cond, ctx_cond, shift, scale, gate)


def row_scale_kernel(lat_ref, ctx_ref, lat_out, ctx_out):
    def scale(ref):
        x = ref[...].astype(F32)
        s = lax.rsqrt(jnp.mean(x * x, axis=-1, keepdims=True) + EPS)
        return jnp.broadcast_to(s, (x.shape[0], 128))

    lat_out[...] = scale(lat_ref)

    @pl.when(pl.program_id(0) == 0)
    def _():
        ctx_out[...] = scale(ctx_ref)


def row_scales(latent, context):
    rows, width = latent.shape
    crows = context.shape[0]
    step = 128
    return pl.pallas_call(
        row_scale_kernel,
        grid=(rows // step,),
        in_specs=[
            pl.BlockSpec((step, width), lambda i: (i, 0)),
            pl.BlockSpec((crows, width), lambda i: (0, 0)),
        ],
        out_specs=[
            pl.BlockSpec((step, 128), lambda i: (i, 0)),
            pl.BlockSpec((crows, 128), lambda i: (0, 0)),
        ],
        out_shape=[
            jax.ShapeDtypeStruct((rows, 128), F32),
            jax.ShapeDtypeStruct((crows, 128), F32),
        ],
        compiler_params=limit(8),
        name="row_scales",
    )(latent, context)


def modulate(i, mods_ref, gain_ref, pieces, m_ref):
    for p in range(PIECES):
        f = i * PIECES + p
        cols = pl.ds(pl.multiple_of(f * 128, 128), 128)
        gain = gain_ref[pl.ds(f, 1)]
        for ref, scale, r, at in pieces:
            n = ref.shape[0]
            shift = mods_ref[i, r * PIECES + p : r * PIECES + p + 1]
            grow = gain * (1.0 + mods_ref[i, (2 + r) * PIECES + p : (2 + r) * PIECES + p + 1])
            x = ref[:, cols].astype(F32)
            m_ref[at : at + n, cols] = (x * scale[...] * grow + shift).astype(BF16)


def project(recv_ref, gain_ref, ls_ref, cs_ref, queue, small, mods_ref, lat_ref, ctx_ref, m_ref, k_ref, v_ref, g_ref, weights):
    parts = mods_ref.shape[0]
    rows = lat_ref.shape[0]
    peers = recv_ref.shape[0] // parts
    for c in queue:
        c.start()
    for c in queue[:small]:
        c.wait()
    for t in range(parts):
        total = recv_ref[t].astype(F32)
        for j in range(1, peers):
            total = total + recv_ref[j * parts + t].astype(F32)
        mods_ref[t] = total
    for i in range(parts):
        queue[small + i].wait()
        modulate(i, mods_ref, gain_ref, ((lat_ref, ls_ref, 0, 0), (ctx_ref, cs_ref, 1, rows)), m_ref)
        cols = slice(i * PIECES * 128, (i + 1) * PIECES * 128)
        step = dot_t(m_ref[:, cols], weights[2][:, cols])
        gates = step if i == 0 else gates + step
    g_ref[...] = gates.astype(BF16)
    wk, wv, _ = weights
    queue[small + parts].wait()
    queue[small + parts + 1].wait()
    k_ref[...] = dot(m_ref[...], wk[...]).astype(BF16)
    v_ref[...] = dot(m_ref[...], wv[...]).astype(BF16)


def maps_kernel(
    recv_hbm, gain_hbm, lat_hbm, ctx_hbm, ls_hbm, cs_hbm, wk_hbm, wv_hbm, wg_hbm, head_ref, wb_ref, db_ref, lr_ref,
    mods_hbm, k_hbm, send_hbm, sv_hbm, gates_hbm,
    recv_ref, gain_ref, lat_ref, ctx_ref, ls_ref, cs_ref, wk, wv, wg,
    mods_ref, k_ref, send_ref, sv_ref, gates_ref, m_ref, v_ref, g_ref, low, inv, uw, kn, in_sems, sems, sv_sems,
):
    parts = mods_ref.shape[0]
    step = lat_ref.shape[1] // parts
    cuts = [slice(i * step, (i + 1) * step) for i in range(parts)]
    loads = [(recv_hbm, recv_ref), (gain_hbm, gain_ref), (ls_hbm, ls_ref), (cs_hbm, cs_ref), (ctx_hbm, ctx_ref)]
    loads += [(wg_hbm, wg)]
    small = len(loads)
    loads += [(lat_hbm.at[:, c], lat_ref.at[:, c]) for c in cuts]
    loads += [(wk_hbm, wk), (wv_hbm, wv)]
    queue = [pltpu.make_async_copy(src, dst, in_sems.at[i]) for i, (src, dst) in enumerate(loads)]
    project(
        recv_ref, gain_ref, ls_ref, cs_ref, queue, small, mods_ref, lat_ref, ctx_ref, m_ref, k_ref, v_ref, g_ref, (wk, wv, wg)
    )

    nblk = (k_ref.shape[0] - 64) // BLOCK
    lats = nblk * BLOCK
    lane = lax.broadcasted_iota(jnp.int32, (1, 8), 1)
    bias = jnp.zeros((1, 8), F32)
    speed = jnp.zeros((1, 8), F32)
    for c in range(4):
        d, h = c // 2, head_ref[0] + c % 2
        bias = jnp.where(lane == c, wb_ref[d, h], jnp.where(lane == 4 + c, db_ref[d, h], bias))
        speed = jnp.where(lane == 4 + c, lr_ref[d, h], speed)
    ri, ci = iotas(BLOCK)
    apart = ri ^ ci
    eye = (ri == ci).astype(F32)
    pre = g_ref[...].astype(F32) + bias
    rates = jax.nn.sigmoid(pre)
    logs = -jnp.exp(speed) * softplus(pre)
    gap = jnp.zeros((pre.shape[0], 120), F32)
    rates = jnp.concatenate([rates, gap], axis=1)
    logs = jnp.concatenate([logs, gap], axis=1)
    below = ri >= ci
    for h in (0, 1):
        kn[h] = unit(k_ref[:, h * HEAD_DIM : (h + 1) * HEAD_DIM])
    strict = (ri > ci, ri < ci)

    def system(slot, gram, d, rate, col, rowv):
        spread = jnp.where(strict[d], col - rowv, 0.0)
        s = jnp.where(strict[d], gram * (-rate) * jnp.exp(spread), 0.0)
        low[slot] = s.astype(BF16)
        inv[slot] = (eye + jnp.where(apart == 1, s, 0.0)).astype(BF16)

    half = BLOCK // 2
    same = apart < half
    crate = jnp.concatenate([rates[lats:]] * 2, axis=0)
    clog = jnp.concatenate([logs[lats:]] * 2, axis=0)
    cfwd = running_sums((below & same).astype(BF16), clog)
    top = lax.broadcasted_iota(jnp.int32, (BLOCK, 1), 0) < half
    cbwd = clog - cfwd + jnp.where(top, cfwd[half - 1 : half], cfwd[BLOCK - 1 :])
    cr = [jnp.where(top, crate[:, 2 * d : 2 * d + 1], crate[:, 2 * d + 1 : 2 * d + 2]) for d in (0, 1)]
    cg = [
        jnp.where(top, c[:, 4 + 2 * d : 5 + 2 * d], c[:, 5 + 2 * d : 6 + 2 * d])
        for d, c in ((0, cfwd), (1, cbwd))
    ]
    cgt = jnp.where(ci == 0, cg[0], cg[1]).T
    ck = [kn[h, lats:] for h in (0, 1)]
    ckk = jnp.concatenate(ck, axis=0)
    cvv = jnp.concatenate(
        [v_ref[lats:, h * HEAD_DIM : (h + 1) * HEAD_DIM].astype(F32) for h in (0, 1)], axis=0
    )
    ckb = ckk.astype(BF16)
    cgram = jnp.where(same, dot_t(ckb, ckb), 0.0)
    for d in (0, 1):
        system(4 * nblk + d, cgram, d, cr[d], cg[d], cgt[d : d + 1])

    keys = [[None] * nblk for _ in (0, 1)]
    for b in range(nblk):
        rows = slice(b * BLOCK, (b + 1) * BLOCK)
        fwd = running_sums(below.astype(BF16), logs[rows])
        bwd = logs[rows] - fwd + fwd[BLOCK - 1 :]
        both = jnp.where(ci < 4, rates[rows], jnp.where(ci < 6, fwd, bwd))
        turned = both.T
        gates_ref[b, 0] = both
        gates_ref[b, 1] = turned
        for h in (0, 1):
            kb = kn[h, rows].astype(BF16)
            gram = dot_t(kb, kb)
            for d in (0, 1):
                c = 2 * d + h
                system(c * nblk + b, gram, d, both[:, c : c + 1], both[:, 4 + c : 5 + c], turned[4 + c : 5 + c])

    count = 4 * nblk + 2

    def level(i, size):
        pick = (apart >= size) & (apart < 2 * size)
        halves = []
        for s in range(count):
            t = inv[s]
            m = jnp.where(pick, low[s], jnp.zeros((), BF16))
            halves.append(dot(t, m).astype(BF16))
        for s in range(count):
            t = inv[s]
            inv[s] = t + dot(halves[s], t).astype(BF16)
        return size * 2

    lax.fori_loop(0, 6, level, jnp.int32(2))

    for d in (0, 1):
        side = jnp.concatenate([cvv * cr[d], ckk * (cr[d] * jnp.exp(cg[d]))], axis=1)
        solved = dot(inv[4 * nblk + d], side.astype(BF16))
        packed = jnp.concatenate([-solved[:, HEAD_DIM:], solved[:, :HEAD_DIM]], axis=1).astype(BF16)
        for h in (0, 1):
            c = 2 * d + h
            rows = slice(h * half, (h + 1) * half)
            end = (h * half + half - 1) if d == 0 else h * half
            last = cg[d][end : end + 1]
            late = ckk[rows] * jnp.exp(last - cg[d][rows])
            ab = t_dot(late.astype(BF16), packed[rows])
            change = (ab[:, :HEAD_DIM] + eye * (jnp.exp(last) - 1.0)).astype(BF16)
            add = ab[:, HEAD_DIM:].T.astype(BF16)
            for s in range(4):
                send_ref[s * 4 + c, BLOCK : 2 * BLOCK] = change
                send_ref[s * 4 + c, 2 * BLOCK + SLICE : 2 * BLOCK + 2 * SLICE] = add[s * SLICE : (s + 1) * SLICE]

    lat_rows = (slice(0, BLOCK), slice(2 * BLOCK, 2 * BLOCK + SLICE))
    ctx_rows = (slice(BLOCK, 2 * BLOCK), slice(2 * BLOCK + SLICE, 2 * BLOCK + 2 * SLICE))
    pairs = [(gates_ref, gates_hbm), (k_ref, k_hbm), (mods_ref, mods_hbm)] + [(send_ref.at[:, r], send_hbm.at[:, r]) for r in ctx_rows]
    waiting = fetches(pairs, sems)

    for b in range(nblk):
        rows = slice(b * BLOCK, (b + 1) * BLOCK)
        both = gates_ref[b, 0]
        for h in (0, 1):
            cols = slice(h * HEAD_DIM, (h + 1) * HEAD_DIM)
            kk = kn[h, rows]
            vv = v_ref[rows, cols].astype(F32)
            for d in (0, 1):
                c = 2 * d + h
                rate = both[:, c : c + 1]
                g = both[:, 4 + c : 5 + c]
                side = jnp.concatenate([kk * (rate * jnp.exp(g)), vv * rate], axis=1).astype(BF16)
                uw[c * nblk + b] = dot(inv[c * nblk + b], side)

    start = jnp.concatenate([eye, jnp.zeros_like(eye)], axis=1)
    states = [start] * 4
    for t in range(nblk):
        for c in range(4):
            d, h = c // 2, c % 2
            b = t if d == 0 else nblk - 1 - t
            rows = slice(b * BLOCK, (b + 1) * BLOCK)
            state = states[c]
            sb = state.astype(BF16)
            sv_ref[c * nblk + b, :BLOCK] = sb
            solved = uw[c * nblk + b]
            moved = dot(solved[:, :HEAD_DIM].astype(BF16), sb)
            fresh = jnp.concatenate(
                [-moved[:, :HEAD_DIM], solved[:, HEAD_DIM:] - moved[:, HEAD_DIM:]], axis=1
            ).astype(BF16)
            sv_ref[c * nblk + b, BLOCK:] = fresh
            g = gates_ref[b, 0][:, 4 + c : 5 + c]
            end = BLOCK - 1 if d == 0 else 0
            last = g[end : end + 1]
            late = (kn[h, rows] * jnp.exp(last - g)).astype(BF16)
            states[c] = state * jnp.exp(last) + t_dot(late, fresh)
        for c in range(4):
            b = c * nblk + (t if c < 2 else nblk - 1 - t)
            copy = pltpu.make_async_copy(sv_ref.at[b], sv_hbm.at[b], sv_sems.at[b])
            copy.start()
            waiting.append(copy)
    for c in range(4):
        change = (states[c][:, :HEAD_DIM] - eye).astype(BF16)
        add = states[c][:, HEAD_DIM:].T.astype(BF16)
        for s in range(4):
            send_ref[s * 4 + c, :BLOCK] = change
            send_ref[s * 4 + c, 2 * BLOCK : 2 * BLOCK + SLICE] = add[s * SLICE : (s + 1) * SLICE]
    late_pairs = [(send_ref.at[:, r], send_hbm.at[:, r]) for r in lat_rows]
    for i, (src, dst) in enumerate(late_pairs):
        copy = pltpu.make_async_copy(src, dst, sems.at[len(pairs) + i])
        copy.start()
        waiting.append(copy)
    for copy in waiting:
        copy.wait()


def chunk_maps(recv, gain, latent, context, ls, cs, wk, wv, wg, head, wb, db, lr, parts):
    rows, width = latent.shape
    every = rows + context.shape[0]
    ncol = wk.shape[1]
    nblk = rows // BLOCK
    count = 4 * nblk
    outs = [
        jax.ShapeDtypeStruct((16, 2 * BLOCK + 2 * SLICE, HEAD_DIM), BF16),
        jax.ShapeDtypeStruct((count, 2 * BLOCK, 2 * HEAD_DIM), BF16),
        jax.ShapeDtypeStruct((nblk, 2, BLOCK, 128), F32),
    ]
    outs = [
        jax.ShapeDtypeStruct((parts, 4 * PIECES, 128), F32),
        jax.ShapeDtypeStruct((every, ncol), BF16),
    ] + outs
    smem = pl.BlockSpec(memory_space=pltpu.SMEM)
    loaded = (recv, gain, latent, context, ls, cs, wk, wv, wg)
    return pl.pallas_call(
        maps_kernel,
        in_specs=[HBM] * 9 + [smem] * 4,
        out_specs=[HBM] * 5,
        out_shape=outs,
        scratch_shapes=[pltpu.VMEM(a.shape, a.dtype) for a in loaded]
        + [pltpu.VMEM(o.shape, o.dtype) for o in outs]
        + [
            pltpu.VMEM((every, width), BF16),
            pltpu.VMEM((every, ncol), BF16),
            pltpu.VMEM((every, wg.shape[0]), BF16),
            pltpu.VMEM((count + 2, BLOCK, BLOCK), BF16),
            pltpu.VMEM((count + 2, BLOCK, BLOCK), BF16),
            pltpu.VMEM((count, BLOCK, 2 * HEAD_DIM), F32),
            pltpu.VMEM((2, every, HEAD_DIM), F32),
            pltpu.SemaphoreType.DMA((parts + 8,)),
            pltpu.SemaphoreType.DMA((7,)),
            pltpu.SemaphoreType.DMA((count,)),
        ],
        compiler_params=limit(60),
        name="chunk_maps",
    )(recv, gain, latent, context, ls, cs, wk, wv, wg, head, wb, db, lr)


def query_kernel(
    mods_ref, gain_ref, lat_ref, ls_ref, wq_ref, k_ref, sv_ref, gates_ref, eff_ref, local_ref, m_ref, q_ref
):
    nblk = q_ref.shape[0] // BLOCK

    def fill(i, carry):
        modulate(i, mods_ref, gain_ref, ((lat_ref, ls_ref, 0, 0),), m_ref)
        return carry

    lax.fori_loop(0, mods_ref.shape[0], fill, 0)
    q_ref[...] = dot(m_ref[...], wq_ref[...]).astype(BF16)
    ri, ci = iotas(BLOCK)
    seen = (ri >= ci, ri <= ci)
    for b in range(nblk):
        rows = slice(b * BLOCK, (b + 1) * BLOCK)
        both = gates_ref[b, 0]
        turned = gates_ref[b, 1]
        for h in (0, 1):
            cols = slice(h * HEAD_DIM, (h + 1) * HEAD_DIM)
            qq = unit(q_ref[rows, cols]) * HEAD_DIM**-0.5
            kb = unit(k_ref[rows, cols]).astype(BF16)
            scores = dot_t(qq.astype(BF16), kb)
            local = None
            for d in (0, 1):
                c = 2 * d + h
                g = both[:, 4 + c : 5 + c]
                spread = jnp.where(seen[d], g - turned[4 + c : 5 + c], 0.0)
                decayed = jnp.where(seen[d], scores * jnp.exp(spread), 0.0)
                side = jnp.concatenate([qq * jnp.exp(g), decayed], axis=1).astype(BF16)
                out = dot(side, sv_ref[c * nblk + b])
                eff_ref[h, rows, d * HEAD_DIM : (d + 1) * HEAD_DIM] = out[:, :HEAD_DIM].astype(BF16)
                local = out[:, HEAD_DIM:] if local is None else local + out[:, HEAD_DIM:]
            local_ref[h, rows] = local


def query_parts(mods, gain, latent, ls, wq, k, sv, gates):
    rows = latent.shape[0]
    return pl.pallas_call(
        query_kernel,
        in_specs=[VMEM] * 8,
        out_specs=[VMEM] * 2,
        out_shape=[
            jax.ShapeDtypeStruct((2, rows, 2 * HEAD_DIM), BF16),
            jax.ShapeDtypeStruct((2, rows, HEAD_DIM), F32),
        ],
        scratch_shapes=[pltpu.VMEM(latent.shape, BF16), pltpu.VMEM((rows, wq.shape[1]), BF16)],
        compiler_params=limit(60),
        name="query_parts",
    )(mods, gain, latent, ls, wq, k, sv, gates)


GROUP = 4


def states_kernel(back_ref, recv_ref, part_ref, out_ref, comp):
    back = back_ref[0]
    peers = recv_ref.shape[0]
    for j in range(peers):
        out_ref[j, SLICE:] = part_ref[...]
    groups = peers // GROUP
    ri, ci = iotas(HEAD_DIM)
    eye = (ri == ci).astype(F32)

    def at(t):
        return jnp.where(back == 1, peers - 1 - t, t)

    def through(rows, weight):
        hi = rows.astype(BF16)
        lo = (rows - hi.astype(F32)).astype(BF16)
        n = rows.shape[0]
        moved = dot_t(jnp.concatenate([hi, lo], axis=0), weight)
        return moved[:n] + moved[n:]

    still = jnp.concatenate([eye, jnp.zeros((SLICE, HEAD_DIM), F32)], axis=0)
    running = [[jnp.zeros_like(still)] * groups for _ in (0, 1)]
    for t in range(GROUP):
        for kind in (0, 1):
            base = BLOCK * (1 - kind)
            extra = 2 * BLOCK + SLICE * (1 - kind)
            for g in range(groups):
                i = at(g * GROUP + t)
                rows = running[kind][g]
                moved = through(rows + still, recv_ref[i, base : base + BLOCK])
                add = recv_ref[i, extra : extra + SLICE].astype(F32)
                rows = rows + moved
                rows = jnp.concatenate([rows[:HEAD_DIM], rows[HEAD_DIM:] + add], axis=0)
                running[kind][g] = rows
                if t < GROUP - 1:
                    comp[kind * peers + g * GROUP + t + 1] = rows

    eye16 = eye.astype(BF16)

    def apply(state, rows):
        hi = state.astype(BF16)
        lo = (state - hi.astype(F32)).astype(BF16)
        both = jnp.concatenate([hi, lo], axis=0)
        weight = jnp.concatenate([rows[:HEAD_DIM].astype(BF16), eye16], axis=0)
        moved = dot(jnp.concatenate([both, both], axis=1), weight)
        return moved[:SLICE] + moved[SLICE:] + rows[HEAD_DIM:]

    state = running[0][0][HEAD_DIM:]
    for g in range(1, groups):
        state = apply(state, running[0][g])
    entries = [state]
    for g in range(groups - 1):
        entries.append(apply(entries[-1], running[1][g]))
    for g in range(groups):
        for t in range(GROUP):
            i = at(g * GROUP + t)
            out = entries[g] if t == 0 else apply(entries[g], comp[peers + g * GROUP + t])
            out_ref[i, :SLICE] = out.astype(BF16)


def entering_states(back, recv, part):
    peers = recv.shape[0]
    return pl.pallas_call(
        states_kernel,
        in_specs=[pl.BlockSpec(memory_space=pltpu.SMEM), VMEM, VMEM],
        out_shape=jax.ShapeDtypeStruct((peers, SLICE + 2 * PIECES, HEAD_DIM), BF16),
        scratch_shapes=[pltpu.VMEM((2 * peers, HEAD_DIM + SLICE, HEAD_DIM), F32)],
        compiler_params=limit(16),
        name="entering_states",
    )(back, recv, part)


def heads_kernel(
    states_hbm, eff_hbm, local_hbm, gain_hbm, out_ref, gate_ref, states_ref, eff_ref, local_ref, gain_ref, sems
):
    pairs = [(states_hbm, states_ref), (gain_hbm, gain_ref)]
    pairs += [(src.at[h], dst.at[h]) for h in (0, 1) for src, dst in ((eff_hbm, eff_ref), (local_hbm, local_ref))]
    copies = fetches(pairs, sems)
    copies[0].wait()
    copies[1].wait()
    for h in (0, 1):
        turned = [
            jnp.concatenate([states_ref[s * 4 + 2 * d + h, :SLICE] for s in range(4)], axis=0) for d in (0, 1)
        ]
        copies[2 + 2 * h].wait()
        copies[3 + 2 * h].wait()
        combined = local_ref[h] + dot_t(eff_ref[h], jnp.concatenate(turned, axis=1))
        scale = lax.rsqrt(jnp.mean(combined * combined, axis=-1, keepdims=True) + EPS)
        out_ref[:, h * HEAD_DIM : (h + 1) * HEAD_DIM] = (combined * scale * gain_ref[...]).astype(BF16)
    gate = states_ref[0, SLICE:].astype(F32)
    for j in range(1, states_ref.shape[0]):
        gate = gate + states_ref[j, SLICE:].astype(F32)
    gate_ref[...] = gate[:PIECES] + gate[PIECES:]


def head_outputs(states, eff, local, gain):
    rows = eff.shape[1]
    arrays = (states, eff, local, gain)
    return pl.pallas_call(
        heads_kernel,
        in_specs=[HBM] * 4,
        out_specs=[VMEM] * 2,
        out_shape=[
            jax.ShapeDtypeStruct((rows, 2 * HEAD_DIM), BF16),
            jax.ShapeDtypeStruct((PIECES, HEAD_DIM), F32),
        ],
        scratch_shapes=[pltpu.VMEM(a.shape, a.dtype) for a in arrays] + [pltpu.SemaphoreType.DMA((6,))],
        compiler_params=limit(60),
        name="head_outputs",
    )(*arrays)


def own_kernel(mine_ref, w_ref, out_ref):
    out_ref[...] = dot(mine_ref[...], w_ref[...])


def update_kernel(sum_ref, other_ref, w_ref, lat_ref, gate_ref, out_ref):
    acc = sum_ref[...] + dot(other_ref[...], w_ref[...])
    for p in range(PIECES):
        cols = slice(p * 128, (p + 1) * 128)
        out_ref[:, cols] = (lat_ref[:, cols].astype(F32) + gate_ref[p : p + 1] * acc[:, cols]).astype(BF16)


def own_half(mine, w):
    return pl.pallas_call(
        own_kernel,
        in_specs=[VMEM] * 2,
        out_specs=VMEM,
        out_shape=jax.ShapeDtypeStruct((mine.shape[0], w.shape[1]), F32),
        compiler_params=limit(16),
        name="own_half",
    )(mine, w)


def update(part, other, w, latent, gate):
    rows = latent.shape[0]
    return pl.pallas_call(
        update_kernel,
        in_specs=[VMEM] * 5,
        out_specs=VMEM,
        out_shape=jax.ShapeDtypeStruct((rows, w.shape[1]), BF16),
        compiler_params=limit(16),
        name="update",
    )(part, other, w, latent, gate)


def body(
    latent,
    context,
    condition,
    context_condition,
    shift_weight,
    scale_weight,
    gate_weight,
    norm_gain,
    query_weight,
    key_weight,
    value_weight,
    write_weight,
    decay_weight,
    write_bias,
    decay_bias,
    log_rate,
    head_gain,
    out_weight,
):
    heads = query_weight.shape[1] // HEAD_DIM
    y, core = lax.axis_index("y"), lax.axis_index("c")
    part = y * 2 + core
    first_head = part * heads
    parts = lax.axis_size(TP)
    peers = lax.axis_size(SP)

    sums, gate_part = partial_sums(
        condition,
        context_condition,
        shift_weight,
        scale_weight,
        gate_weight,
        peers * parts,
    )
    sums = lax.all_to_all(sums, ALL, split_axis=0, concat_axis=0, tiled=True)

    def own(a):
        return lax.dynamic_slice_in_dim(a, first_head, heads, a.ndim - 1)

    gates_w = jnp.concatenate(
        [own(write_weight).reshape(-1, 2 * heads), own(decay_weight).reshape(-1, 2 * heads)], axis=1
    ).T

    ls, cs = row_scales(latent, context)
    gain = norm_gain.reshape(-1, 128)
    head = first_head.astype(jnp.int32).reshape(1)
    mods, k, send, sv, gates = chunk_maps(
        sums,
        gain,
        latent,
        context,
        ls,
        cs,
        key_weight,
        value_weight,
        gates_w,
        head,
        write_bias,
        decay_bias,
        log_rate,
        parts,
    )
    maps = lax.all_to_all(send, SP, split_axis=0, concat_axis=0, tiled=True)
    eff, local = query_parts(mods, gain, latent, ls, query_weight, k, sv, gates)
    columns = out_weight.shape[1]
    residual = lax.dynamic_slice_in_dim(latent, part * columns, columns, 1)
    block = head_gain.shape[0] * heads

    def ring_rows(which):
        places = [lax.rem(y + off, 4) * 2 + which for off in (0, 3, 1, 2)]
        return jnp.concatenate([lax.dynamic_slice_in_dim(out_weight, p * block, block, 0) for p in places])

    maps, eff, local, residual, w_mine, w_other = lax.optimization_barrier(
        (maps, eff, local, residual, ring_rows(core), ring_rows(1 - core))
    )
    chain = lax.rem(lax.axis_index("x"), 4)
    back = (chain // 2).astype(jnp.int32).reshape(1)
    starts = entering_states(back, maps, gate_part)
    states = lax.all_to_all(starts, SP, split_axis=0, concat_axis=0, tiled=True)
    head_out, gate_row = head_outputs(states, eff, local, head_gain.reshape(1, -1))

    n = lax.axis_size("y")
    up = [(i, (i + 1) % n) for i in range(n)]
    down = [(i, (i - 1) % n) for i in range(n)]
    cut = head_out.shape[0] // 2
    below = lax.ppermute(head_out, "y", up)
    above = lax.ppermute(head_out, "y", down)
    far_a = lax.ppermute(below[:cut], "y", up)
    far_b = lax.ppermute(above[cut:], "y", down)
    mine = jnp.concatenate([head_out, below, above, jnp.concatenate([far_a, far_b])], axis=1)
    other = lax.ppermute(mine, "c", [(0, 1), (1, 0)])
    half = own_half(mine, w_mine)
    return update(half, other, w_other, residual, gate_row)


def solution(mesh):
    torus = Mesh(mesh.devices.reshape(4, 4, 4, 2), ALL)
    placed = (
        P(SP, None),
        P(SP, None),
        P(SP),
        P(SP),
        P(SP, TP),
        P(SP, TP),
        P(SP, TP),
        P(),
        P(None, TP),
        P(None, TP),
        P(None, TP),
        P(),
        P(),
        P(),
        P(),
        P(),
        P(),
        P(None, TP),
    )
    return jax.shard_map(body, mesh=torus, in_specs=placed, out_specs=P(SP, TP), check_vma=False)
```
